32 devices in a mesh: sp: 8 (over z, y), tp: 4 (over x, core).
Axes of the slice: x: 2, y: 2, z: 4, core: 2. Of those that a mesh axis runs over, the one named last changes fastest.
Arguments:
- tokens: bfloat16 [8192, 2048], P('sp', 'tp'), may hold values from -16 to 16
- mix_gain: float32 [2048], replicated, may hold values from 0.1 to 1.9
- query_weight: bfloat16 [2048, 1024], P(None, 'tp'), may hold values from -0.125 to 0.125
- key_weight: bfloat16 [2048, 1024], P(None, 'tp'), may hold values from -0.125 to 0.125
- value_weight: bfloat16 [2048, 1024], P(None, 'tp'), may hold values from -0.125 to 0.125
- outer_gate_weight: bfloat16 [2048, 1024], P(None, 'tp'), may hold values from -0.125 to 0.125
- inner_gate_weight: bfloat16 [2048, 1024], P(None, 'tp'), may hold values from -0.125 to 0.125
- conv_input_weight: bfloat16 [2048, 1024], P(None, 'tp'), may hold values from -0.125 to 0.125
- query_gain: float32 [64], replicated, may hold values from 0.6 to 10
- key_gain: float32 [64], replicated, may hold values from 0.6 to 10
- gate_totals: float32 [8192, 16], P('sp', 'tp'), may hold values from -2048 to 0, as said below
- conv_taps: float32 [3, 1024], P(None, 'tp'), may hold values from -3 to 3
- attn_out_gain: float32 [1024], P('tp'), may hold values from 0.1 to 1.9
- conv_out_gain: float32 [1024], P('tp'), may hold values from 0.1 to 1.9
- attn_out_weight: bfloat16 [1024, 2048], P('tp'), may hold values from -0.125 to 0.125
- conv_out_weight: bfloat16 [1024, 2048], P('tp'), may hold values from -0.125 to 0.125
Outputs:
- mixed: bfloat16 [8192, 2048], P(('sp', 'tp'))
The draws below stay inside these ranges and needn't reach their ends.
Inputs may be any that keep to these rules, and one draw needn't show every extreme that they name: `gate_totals`: in every head the values never rise from one position to the next.
All inputs are finite; a program needn't handle non-finite values.
Results may differ from the reference program's by a relative error of at most 0.015.
The reference program's roundings to bfloat16 on the way count: a program that leaves them out, or rounds other values in their place, can miss the bound.
Values may be sent and summed in bfloat16 or wider, within the bound.
A program may use at most 64 MiB of HBM per device.

```python
import math
import jax
import jax.numpy as jnp
from jax import lax

D = 2048
HEAD_DIM = 64
ATTENTION_HEADS = 16
CONV_K = 3
TOK_DEV = 1024
ATTN_WIDTH = 1024
CONV_WIDTH = 1024
SEQUENCE_TOKENS = 8192
N_TP = 4


def draw_tokens(key, part):
    random_subkeys = jax.random.split(jax.random.fold_in(key, 101), 2)
    column = jnp.arange(D, dtype=jnp.float32) / D
    column_scale = 0.5 * jnp.exp(math.log(4.0) * column) * jax.random.uniform(random_subkeys[1], (D,), jnp.float32, 0.7, 1.4)
    normal_part = jax.random.normal(random_subkeys[0], (SEQUENCE_TOKENS, D), jnp.float32)
    return jnp.clip(normal_part * column_scale, -16.0, 16.0).astype(jnp.bfloat16)


def focus_gain(key):
    gain = jax.random.uniform(key, (HEAD_DIM,), jnp.float32, 0.6, 1.4)
    return gain


def draw_query_gain(key, part):
    return focus_gain(jax.random.fold_in(key, 211))


def draw_key_gain(key, part):
    return focus_gain(jax.random.fold_in(key, 307))


def draw_gate_totals(key, part):
    random_subkeys = jax.random.split(jax.random.fold_in(key, 401), 7)
    order = jax.random.permutation(random_subkeys[0], ATTENTION_HEADS)
    fast_path = order < ATTENTION_HEADS // 2
    slow_total = jax.random.uniform(random_subkeys[1], (ATTENTION_HEADS,), jnp.float32, 0.15, 0.5)
    quick_reach = jnp.exp(jax.random.uniform(random_subkeys[2], (ATTENTION_HEADS,), jnp.float32, math.log(30.0), math.log(100.0)))
    base_rate = jnp.where(fast_path, 1.0 / quick_reach, slow_total / SEQUENCE_TOKENS)
    block_factor = jnp.exp(jax.random.uniform(random_subkeys[3], (SEQUENCE_TOKENS // TOK_DEV, 1), jnp.float32, math.log(0.5), math.log(2.0)))
    block_rate = jnp.repeat(block_factor, TOK_DEV, axis=0)
    jitter = jnp.exp(jax.random.uniform(random_subkeys[4], (SEQUENCE_TOKENS, ATTENTION_HEADS), jnp.float32, math.log(0.5), math.log(2.0)))
    per_step_loss = base_rate[None, :] * block_rate * jitter
    spike_position = jax.random.randint(random_subkeys[5], (2,), 0, SEQUENCE_TOKENS)
    spike_hit = jnp.any(jnp.arange(SEQUENCE_TOKENS)[:, None] == spike_position[None, :], axis=1)
    spike_loss = jax.random.uniform(random_subkeys[6], (SEQUENCE_TOKENS, ATTENTION_HEADS), jnp.float32, 0.22, 0.51)
    per_step_loss = per_step_loss + jnp.where(spike_hit[:, None] & jnp.logical_not(fast_path)[None, :], spike_loss, 0.0)
    return -jnp.cumsum(per_step_loss, axis=0)


def block_levels(stream_key, shape, cuts, low, top_value):
    level, own = 1.0, jax.random.fold_in(stream_key, 6)
    for position, shards_of in cuts:
        draws = jnp.exp(jax.random.uniform(jax.random.fold_in(own, position), (shards_of,), jnp.float32, low / len(cuts), top_value / len(cuts)))
        level = level * jnp.repeat(draws, shape[position] // shards_of).reshape([-1 if axis == position else 1 for axis in range(len(shape))])
    return level


def centred(stream_key, shape, deviation, most, cuts=(), kind=jnp.bfloat16):
    array = deviation * jax.random.normal(stream_key, shape, jnp.float32)
    if cuts:
        array = array * block_levels(stream_key, shape, cuts, -0.22, 0.18)
    return jnp.clip(array, -most, most).astype(kind)


def setup_inputs(seed: int = 0) -> dict:
    key_of = jax.random.split(jax.random.key(seed), 17)
    return {
        "tokens": draw_tokens(jax.random.fold_in(key_of[16], 71), 0),
        "mix_gain": jnp.clip(1.0 + 0.18 * jax.random.normal(key_of[1], (D,), jnp.float32), 0.1, 1.9),
        "query_weight": centred(key_of[2], (D, ATTN_WIDTH), D ** -0.5, 0.125, ((1, 4),)),
        "key_weight": centred(key_of[3], (D, ATTN_WIDTH), D ** -0.5, 0.125, ((1, 4),)),
        "value_weight": centred(key_of[4], (D, ATTN_WIDTH), D ** -0.5, 0.125, ((1, 4),)),
        "outer_gate_weight": centred(key_of[5], (D, CONV_WIDTH), D ** -0.5, 0.125, ((1, 4),)),
        "inner_gate_weight": centred(key_of[6], (D, CONV_WIDTH), D ** -0.5, 0.125, ((1, 4),)),
        "conv_input_weight": centred(key_of[7], (D, CONV_WIDTH), D ** -0.5, 0.125, ((1, 4),)),
        "query_gain": draw_query_gain(jax.random.fold_in(key_of[16], 71), 0),
        "key_gain": draw_key_gain(jax.random.fold_in(key_of[16], 71), 0),
        "gate_totals": draw_gate_totals(jax.random.fold_in(key_of[16], 71), 0),
        "conv_taps": centred(key_of[11], (CONV_K, CONV_WIDTH), 0.6, 3.0, ((1, 4),), jnp.float32),
        "attn_out_gain": jnp.clip(1.0 + 0.18 * jax.random.normal(key_of[12], (ATTN_WIDTH,), jnp.float32), 0.1, 1.9),
        "conv_out_gain": jnp.clip(1.0 + 0.18 * jax.random.normal(key_of[13], (CONV_WIDTH,), jnp.float32), 0.1, 1.9),
        "attn_out_weight": centred(key_of[14], (ATTN_WIDTH, D), (ATTN_WIDTH + CONV_WIDTH) ** -0.5, 0.125, ((0, 4),)),
        "conv_out_weight": centred(key_of[15], (CONV_WIDTH, D), (ATTN_WIDTH + CONV_WIDTH) ** -0.5, 0.125, ((0, 4),)),
    }


NORM_EPSILON = 1e-06

def head_norm(values, head_dim, gain):
    row_count = values.shape[0]
    grouped = values.reshape(row_count, -1, head_dim)
    normed = grouped * lax.rsqrt(lax.optimization_barrier(jnp.mean(grouped * grouped, axis=2, keepdims=True)) + NORM_EPSILON)
    return (normed * gain.reshape(-1, head_dim)).reshape(row_count, -1)

def settle(values):
    return lax.optimization_barrier(values.astype(jnp.bfloat16)).astype(jnp.float32)

def reference(tokens, mix_gain, query_weight, key_weight, value_weight, outer_gate_weight, inner_gate_weight, conv_input_weight, query_gain, key_gain, gate_totals, conv_taps, attn_out_gain, conv_out_gain, attn_out_weight, conv_out_weight):
    widened = tokens.astype(jnp.float32)
    row_scale = lax.rsqrt(lax.optimization_barrier(jnp.sum(widened * widened, axis=1, keepdims=True)) / D + NORM_EPSILON)
    scaled = (widened * mix_gain).astype(jnp.bfloat16)

    def project(weight):
        return row_scale * jnp.dot(scaled, weight, preferred_element_type=jnp.float32)
    queries = settle(head_norm(project(query_weight), HEAD_DIM, query_gain))
    key_rows = settle(head_norm(project(key_weight), HEAD_DIM, key_gain))
    value_rows = settle(project(value_weight))
    query_span = math.gcd(SEQUENCE_TOKENS, 512)
    score_scale = HEAD_DIM ** (-0.5)
    positions = jnp.arange(SEQUENCE_TOKENS, dtype=jnp.int32)

    def one_head(head_index):
        offset = (head_index * HEAD_DIM).astype(jnp.int32)
        head_queries = lax.dynamic_slice_in_dim(queries, offset, HEAD_DIM, 1)
        head_keys = lax.dynamic_slice_in_dim(key_rows, offset, HEAD_DIM, 1)
        head_values = lax.dynamic_slice_in_dim(value_rows, offset, HEAD_DIM, 1)
        head_gates = lax.dynamic_slice_in_dim(gate_totals, head_index.astype(jnp.int32), 1, 1)[:, 0]

        def one_block(block_index):
            start = (block_index * query_span).astype(jnp.int32)
            block_queries = lax.dynamic_slice_in_dim(head_queries, start, query_span, 0)
            block_gates = lax.dynamic_slice_in_dim(head_gates, start, query_span, 0)
            scores = jnp.dot(block_queries, head_keys.T, precision=lax.Precision.HIGHEST) * score_scale
            scores = scores + block_gates[:, None] - head_gates[None, :]
            allowed = positions[None, :] <= (start + jnp.arange(query_span, dtype=jnp.int32))[:, None]
            row_max = lax.optimization_barrier(jnp.max(jnp.where(allowed, scores, -jnp.inf), axis=1, keepdims=True))
            weights = settle(jnp.where(allowed, jnp.exp(scores - row_max), 0.0))
            return jnp.dot(weights, head_values, precision=lax.Precision.HIGHEST)
        blocks = lax.map(one_block, jnp.arange(SEQUENCE_TOKENS // query_span, dtype=jnp.int32))
        return blocks.reshape(SEQUENCE_TOKENS, HEAD_DIM)
    attended = lax.map(one_head, jnp.arange(ATTENTION_HEADS, dtype=jnp.int32))
    attended = jnp.transpose(attended, (1, 0, 2)).reshape(SEQUENCE_TOKENS, ATTN_WIDTH)
    attn_mixed = head_norm(attended, HEAD_DIM, attn_out_gain).astype(jnp.bfloat16)
    gated = settle(project(inner_gate_weight) * project(conv_input_weight))
    padded = jnp.concatenate([jnp.zeros((CONV_K - 1, CONV_WIDTH), jnp.float32), gated], axis=0)
    convolved = conv_taps[0] * padded[0:SEQUENCE_TOKENS]
    for tap_index in range(1, CONV_K):
        convolved = convolved + conv_taps[tap_index] * padded[tap_index:tap_index + SEQUENCE_TOKENS]
    conv_mixed = head_norm(project(outer_gate_weight) * convolved, HEAD_DIM, conv_out_gain).astype(jnp.bfloat16)
    attn_slice = ATTN_WIDTH // N_TP
    conv_slice = CONV_WIDTH // N_TP
    total = jnp.zeros((SEQUENCE_TOKENS, D), jnp.float32)
    for slice_index in range(N_TP):
        attn_lo = slice_index * attn_slice
        conv_lo = slice_index * conv_slice
        partial_value = jnp.dot(attn_mixed[:, attn_lo:attn_lo + attn_slice], attn_out_weight[attn_lo:attn_lo + attn_slice], preferred_element_type=jnp.float32)
        partial_value = partial_value + jnp.dot(conv_mixed[:, conv_lo:conv_lo + conv_slice], conv_out_weight[conv_lo:conv_lo + conv_slice], preferred_element_type=jnp.float32)
        total = total + settle(partial_value)
    return total.astype(jnp.bfloat16)
```

```python
import functools

import jax
import jax.numpy as jnp
from jax import lax
from jax.experimental import pallas as pl
from jax.experimental.pallas import tpu as pltpu
from jax.sharding import PartitionSpec as P

NORM_EPSILON = 1e-06
MESH = pl.DeviceIdType.MESH
CORES = 2
LANES = 128
VMEM = pltpu.VMEM


def greet(devices):
    barrier = pltpu.get_barrier_semaphore()
    for sp, tp in devices:
        pl.semaphore_signal(barrier, inc=1, device_id=(sp, tp), device_id_type=MESH)
    pl.semaphore_wait(barrier, len(devices))


def mesh_copy(src, dst, send, recv, device):
    return pltpu.make_async_remote_copy(
        src, dst, send, recv, device_id=device, device_id_type=MESH
    )


def front_kernel(
    plan, tokens_ref, mix_ref, query_gain_ref, key_gain_ref, taps_ref, conv_gain_ref, side_ref, *refs
):
    sp_count, tp_count, head_count, head_dim, chunk = plan
    query_gain = jnp.concatenate([query_gain_ref[...]] * plan[2], axis=1)
    key_gain = jnp.concatenate([key_gain_ref[...]] * plan[2], axis=1)
    weight_refs = refs[:6]
    kv_out, query_out, side_out, conv_out = refs[6:10]
    (
        weights, gathered, scaled, kv_send, query_send, outer, padded, edge_send, edge_recv,
        weight_sem, own_sem, cross_send, mate_send, tok_pass_send, tok_recv,
        kv_ssem, kv_rsem, query_ssem, query_rsem, side_ssem, side_rsem,
        kv_psem, kv_prsem, query_psem, query_prsem, side_psem, side_prsem, local, edge_sem,
    ) = refs[10:]
    sp = lax.axis_index("sp")
    tp = lax.axis_index("tp")
    core = lax.rem(tp, CORES)
    mate = tp + 1 - 2 * core
    chips = tp_count // CORES
    targets = sp_count // CORES
    share = targets // head_count
    rows, features = tokens_ref.shape
    chunks = rows // chunk
    half = chunk // 2
    width = head_count * head_dim
    order = [chunks - 1] + list(range(chunks - 1))

    loads = [
        pltpu.make_async_copy(ref, weights.at[index], weight_sem.at[index])
        for index, ref in enumerate(weight_refs)
    ]
    for load in loads:
        load.start()
    mine = pltpu.make_async_copy(tokens_ref, gathered.at[tp], own_sem)
    mine.start()
    padded[0:8, :] = jnp.zeros((8, width), jnp.float32)
    greet(
        [(lax.rem(sp + step, sp_count), tp) for step in range(1, sp_count)]
        + [(sp, mate)]
        + [(sp, lax.rem(tp + CORES * step, tp_count)) for step in range(1, chips)]
    )

    def block(number):
        return pl.ds(number * chunk, chunk)

    def to_mate(number):
        return mesh_copy(
            tokens_ref.at[block(number)], gathered.at[tp, block(number)], mate_send.at[number],
            tok_recv.at[tp, number], (sp, mate),
        )

    def across(step, number):
        return mesh_copy(
            tokens_ref.at[block(number)], gathered.at[tp, block(number)],
            cross_send.at[step - 1, number], tok_recv.at[tp, number],
            (sp, lax.rem(tp + CORES * step, tp_count)),
        )

    def token_pass(step, number):
        other = lax.rem(tp + CORES * step, tp_count)
        return mesh_copy(
            gathered.at[other, block(number)], gathered.at[other, block(number)],
            tok_pass_send.at[step - 1, number], tok_recv.at[other, number], (sp, mate),
        )

    def token_arrival(source, number):
        return mesh_copy(
            tokens_ref.at[block(number)], gathered.at[source, block(number)], mate_send.at[number],
            tok_recv.at[source, number], (sp, mate),
        )

    for number in order:
        for step in range(1, chips):
            across(step, number).start()
        to_mate(number).start()

    owner = core == sp // targets

    def target_of(step):
        at = lax.rem(sp + 1 + step, targets)
        return at // share, core * targets + at

    def side_copy(step, head, target):
        return mesh_copy(
            side_ref.at[head], side_out.at[sp], side_ssem.at[step], side_rsem.at[sp], (target, tp)
        )

    def kv_copy(step, number, head, target):
        return mesh_copy(
            kv_send.at[head, block(number)], kv_out.at[sp, block(number)],
            kv_ssem.at[step, number], kv_rsem.at[sp, number], (target, tp),
        )

    def query_copy(step, number, head, target):
        at = pl.ds(number * half, half)
        return mesh_copy(
            query_send.at[head, at], query_out.at[sp, at],
            query_ssem.at[step, number], query_rsem.at[sp, number], (target, tp),
        )

    def kept(number, head):
        at = pl.ds(number * half, half)
        return (
            pltpu.make_async_copy(
                kv_send.at[head, block(number)], kv_out.at[sp, block(number)], local.at[0, number]
            ),
            pltpu.make_async_copy(
                query_send.at[head, at], query_out.at[sp, at], local.at[1, number]
            ),
        )

    def kept_side(head):
        return pltpu.make_async_copy(side_ref.at[head], side_out.at[sp], local.at[2, 0])

    for step in range(targets):
        head, target = target_of(step)

        @pl.when(target != sp)
        def _():
            side_copy(step, head, target).start()

        @pl.when(target == sp)
        def _():
            kept_side(head).start()

    ones_row = lax.broadcasted_iota(jnp.int32, (width, width), 0) // head_dim
    ones_column = lax.broadcasted_iota(jnp.int32, (width, width), 1) // head_dim
    spread = jnp.where(ones_row == ones_column, 1.0 / head_dim, 0.0).astype(jnp.bfloat16)

    def normed(values, gain):
        squares = values * values
        high = squares.astype(jnp.bfloat16)
        low = (squares - high.astype(jnp.float32)).astype(jnp.bfloat16)
        mean = jnp.dot(high, spread, preferred_element_type=jnp.float32)
        mean = mean + jnp.dot(low, spread, preferred_element_type=jnp.float32)
        return values * lax.rsqrt(mean + NORM_EPSILON) * gain

    mine.wait()
    for load in loads:
        load.wait()
    for number in order:
        here = block(number)
        for step in range(1, chips):
            token_arrival(lax.rem(tp + CORES * step, tp_count), number).wait_recv()
            token_pass(step, number).start()
        token_arrival(mate, number).wait_recv()
        for step in range(1, chips):
            token_arrival(lax.rem(mate + CORES * step, tp_count), number).wait_recv()
        total = jnp.zeros((chunk, 1), jnp.float32)
        for source in range(tp_count):
            part = gathered[source, here, :].astype(jnp.float32)
            at = slice(source * features, (source + 1) * features)
            total = total + jnp.sum(part * part, axis=1, keepdims=True)
            scaled[:, at] = (part * mix_ref[:, at]).astype(jnp.bfloat16)
        row_scale = lax.rsqrt(total / (tp_count * features) + NORM_EPSILON)

        def project(index):
            product = jnp.dot(scaled[...], weights[index], preferred_element_type=jnp.float32)
            return product * row_scale

        keys = normed(project(1), key_gain).astype(jnp.bfloat16)
        values = project(2)
        queries = normed(project(0), query_gain).astype(jnp.bfloat16)
        queries = queries.astype(jnp.float32) * head_dim ** (-0.5)
        for head in range(head_count):
            at = slice(head * head_dim, (head + 1) * head_dim)
            kv_send[head, pl.ds(number * chunk, half), :] = jnp.concatenate(
                [keys[:half, at], keys[half:, at]], axis=1
            )
        for side in range(2):
            rows_of = slice(side * half, (side + 1) * half)
            for first in range(0, width, LANES):
                at = slice(first, first + LANES)
                flipped_values = values[rows_of, at].T.astype(jnp.bfloat16)
                flipped_queries = queries[rows_of, at].T.astype(jnp.bfloat16)
                for inner in range(LANES // head_dim):
                    head = first // head_dim + inner
                    piece_of = slice(inner * head_dim, (inner + 1) * head_dim)
                    kv_send[
                        head, pl.ds(number * chunk + half + side * head_dim, head_dim), :
                    ] = flipped_values[piece_of]
                    query_send[
                        head, pl.ds(number * half + side * head_dim, head_dim), :
                    ] = flipped_queries[piece_of]
        for step in range(targets):
            head, target = target_of(step)

            @pl.when(target != sp)
            def _():
                kv_copy(step, number, head, target).start()
                query_copy(step, number, head, target).start()

            @pl.when(target == sp)
            def _():
                for copy in kept(number, head):
                    copy.start()

        outer[here, :] = project(3)
        gated = (project(4) * project(5)).astype(jnp.bfloat16)
        padded[pl.ds(8 + number * chunk, chunk), :] = gated.astype(jnp.float32)
        if number == chunks - 1:
            edge_send[...] = gated[chunk - 16 :, :]

            @pl.when(sp < sp_count - 1)
            def _():
                mesh_copy(
                    edge_send, edge_recv, edge_sem.at[0], edge_sem.at[1],
                    (lax.rem(sp + 1, sp_count), tp),
                ).start()

    edge = mesh_copy(
        edge_send, edge_recv, edge_sem.at[0], edge_sem.at[1], (lax.rem(sp + 1, sp_count), tp)
    )

    @pl.when(sp > 0)
    def _():
        edge.wait_recv()
        padded[0:8, :] = edge_recv[8:16, :].astype(jnp.float32)

    taps = taps_ref.shape[0]
    for number in range(chunks):
        convolved = jnp.zeros((chunk, width), jnp.float32)
        for tap in range(taps):
            at = pl.ds(8 - taps + 1 + tap + number * chunk, chunk)
            convolved = convolved + taps_ref[tap : tap + 1, :] * padded[at, :]
        conv_out[block(number), :] = normed(
            outer[block(number), :] * convolved, conv_gain_ref[...]
        ).astype(jnp.bfloat16)

    def kv_pass(source, number):
        return mesh_copy(
            kv_out.at[source, block(number)], kv_out.at[source, block(number)],
            kv_psem.at[source, number], kv_prsem.at[source, number], (sp, mate),
        )

    def query_pass(source, number):
        at = pl.ds(number * half, half)
        return mesh_copy(
            query_out.at[source, at], query_out.at[source, at],
            query_psem.at[source, number], query_prsem.at[source, number], (sp, mate),
        )

    def side_pass(source):
        return mesh_copy(
            side_out.at[source], side_out.at[source], side_psem.at[source], side_prsem.at[source],
            (sp, mate),
        )

    sources = [lax.rem(sp + step, sp_count) for step in range(sp_count)]

    @pl.when(owner)
    def _():
        for step, source in enumerate(sources):
            if step == 0:
                kept_side(0).wait()
            else:
                mesh_copy(
                    side_ref.at[0], side_out.at[source], side_ssem.at[0], side_rsem.at[source],
                    (sp, mate),
                ).wait_recv()
            side_pass(source).start()
        for number in order:
            at = pl.ds(number * half, half)
            for step, source in enumerate(sources):
                if step == 0:
                    for copy in kept(number, 0):
                        copy.wait()
                else:
                    mesh_copy(
                        kv_send.at[0, block(number)], kv_out.at[source, block(number)],
                        kv_ssem.at[0, number], kv_rsem.at[source, number], (sp, mate),
                    ).wait_recv()
                    mesh_copy(
                        query_send.at[0, at], query_out.at[source, at],
                        query_ssem.at[0, number], query_rsem.at[source, number], (sp, mate),
                    ).wait_recv()
                kv_pass(source, number).start()
                query_pass(source, number).start()
        for source in sources:
            side_pass(source).wait_send()
            for number in order:
                kv_pass(source, number).wait_send()
                query_pass(source, number).wait_send()

    @pl.when(jnp.logical_not(owner))
    def _():
        for source in sources:
            side_pass(source).wait_recv()
            for number in order:
                kv_pass(source, number).wait_recv()
                query_pass(source, number).wait_recv()

    for step in range(targets):
        head, target = target_of(step)

        @pl.when(target != sp)
        def _():
            side_copy(step, head, target).wait_send()
            for number in order:
                kv_copy(step, number, head, target).wait_send()
                query_copy(step, number, head, target).wait_send()

    for number in order:
        to_mate(number).wait_send()
        for step in range(1, chips):
            across(step, number).wait_send()
            token_pass(step, number).wait_send()

    @pl.when(sp < sp_count - 1)
    def _():
        edge.wait_send()


def front(tokens, mix_gain, query_gain, key_gain, taps, conv_gain, sides, weights, head_dim, piece):
    sp_count = lax.axis_size("sp")
    tp_count = lax.axis_size("tp")
    rows, features = tokens.shape
    width = weights[0].shape[1]
    heads = width // head_dim
    chunk = 2 * LANES
    chunks = rows // chunk
    chips = tp_count // CORES
    targets = sp_count // CORES
    bf16 = jnp.bfloat16
    dma = pltpu.SemaphoreType.DMA
    across = (max(chips - 1, 1), chunks)
    vmem = pl.BlockSpec(memory_space=VMEM)
    return pl.pallas_call(
        functools.partial(front_kernel, (sp_count, tp_count, heads, head_dim, chunk)),
        out_shape=(
            jax.ShapeDtypeStruct((sp_count, rows, LANES), bf16),
            jax.ShapeDtypeStruct((sp_count, rows // 2, LANES), bf16),
            jax.ShapeDtypeStruct((sp_count,) + sides.shape[1:], sides.dtype),
            jax.ShapeDtypeStruct((rows, width), bf16),
        ),
        in_specs=[vmem] * 7 + [pl.BlockSpec(memory_space=pl.ANY)] * 6,
        out_specs=(vmem,) * 4,
        scratch_shapes=[
            VMEM((6,) + weights[0].shape, bf16),
            VMEM((tp_count, rows, features), bf16),
            VMEM((chunk, tp_count * features), bf16),
            VMEM((heads, rows, LANES), bf16),
            VMEM((heads, rows // 2, LANES), bf16),
            VMEM((rows, width), jnp.float32),
            VMEM((rows + 8, width), jnp.float32),
            VMEM((16, width), bf16),
            VMEM((16, width), bf16),
            dma((6,)), dma, dma(across), dma((chunks,)), dma(across), dma((tp_count, chunks)),
            dma((targets, chunks)), dma((sp_count, chunks)),
            dma((targets, chunks)), dma((sp_count, chunks)),
            dma((targets,)), dma((sp_count,)),
            dma((sp_count, chunks)), dma((sp_count, chunks)),
            dma((sp_count, chunks)), dma((sp_count, chunks)),
            dma((sp_count,)), dma((sp_count,)),
            dma((3, chunks)), dma((2,)),
        ],
        compiler_params=pltpu.CompilerParams(
            collective_id=0, has_side_effects=True, vmem_limit_bytes=56 * 1024 * 1024
        ),
    )(tokens, mix_gain, query_gain, key_gain, taps, conv_gain, sides, *weights)


def rear_kernel(
    plan, query_ref, kv_ref, side_ref, conv_ref, attn_weight, conv_weight, out_ref, done, landed,
    rhs, gates, scores_a, scores_b, flipped, attn, partial, keep, mate_out, mate_in, link_out, link_in, send, recv, local, mate_ssem,
    mate_rsem, link_ssem, link_rsem
):
    sp_count, tp_count, head_dim, piece, sub = plan
    sp = lax.axis_index("sp")
    tp = lax.axis_index("tp")
    core = lax.rem(tp, CORES)
    mate = tp + 1 - 2 * core
    chips = tp_count // CORES
    first = tp - core
    targets = sp_count // CORES
    rows, width = conv_ref.shape
    pieces = rows // piece
    share = pieces // CORES
    block_rows = rows // tp_count
    half = LANES
    chunk = 2 * half
    phases = min(2, piece // half)
    tile = piece // phases
    slabs = piece // half
    span = 256
    subs = block_rows // phases // sub
    greet(
        [
            (lax.rem(sp + step, sp_count), first + lax.rem(core + other, CORES))
            for step in range(sp_count)
            for other in range(CORES)
            if step or other
        ]
        + [(sp, lax.rem(tp + CORES * step, tp_count)) for step in range(1, chips)]
    )
    home = sp // targets
    slot = lax.rem(sp, targets) * CORES + core
    home_here = home == core
    place_here = lax.rem(sp, share) * CORES + core
    bf16 = jnp.bfloat16
    both_tiles = 2 * tile
    gain_tile = jnp.broadcast_to(side_ref[0, rows // LANES : rows // LANES + 1, :], (LANES, LANES))
    gain = gain_tile.T[:head_dim, 0:1]

    def pieces_of(values):
        high = values.astype(bf16).astype(jnp.float32)
        middle = (values - high).astype(bf16).astype(jnp.float32)
        low = (values - high - middle).astype(bf16).astype(jnp.float32)
        return high, middle, low

    def gate_columns(source, _):
        cuts = pieces_of(-side_ref[source, : rows // LANES, :])
        for number in range(rows // chunk):
            lines = [
                cut[2 * number + side : 2 * number + side + 1, :] for side in range(2) for cut in cuts
            ]
            lines.append(jnp.zeros((LANES - len(lines), LANES), jnp.float32))
            gates[source, number * half : (number + 1) * half, :] = (
                jnp.concatenate(lines, axis=0).T.astype(bf16)
            )
        return 0

    lax.fori_loop(0, sp_count, gate_columns, 0)

    def away(phase, source):
        return mesh_copy(
            done.at[phase, source], landed.at[phase, slot], send.at[phase, source],
            recv.at[phase, slot], (source, first + home),
        )

    def stay(phase, source, index):
        return pltpu.make_async_copy(
            done.at[phase, source], landed.at[phase, index], local.at[phase]
        )

    def queries_of(phase, source, spot):
        parts = []
        for slab in range(phase, slabs, phases):
            begin = pl.multiple_of((spot * slabs + slab) * head_dim, head_dim)
            parts.append(query_ref[source, pl.ds(begin, head_dim), :])
        return jnp.concatenate(parts, axis=1)

    def set_queries(phase, even, even_spot, odd, odd_spot):
        queries = jnp.concatenate(
            [queries_of(phase, even, even_spot), queries_of(phase, odd, odd_spot)], axis=1
        )
        empty = jnp.zeros_like(queries)
        row = lax.broadcasted_iota(jnp.int32, (LANES, both_tiles), 0)
        for side in range(2):
            ones = jnp.logical_and(row >= 3 * side, row < 3 * side + 3)
            stacked = [queries, empty] if side == 0 else [empty, queries]
            rhs[side, :, :] = jnp.concatenate(
                stacked + [jnp.where(ones, 1.0, 0.0).astype(bf16)], axis=0
            )

    def score(source, side, scores, top, limit):
        key_rows = jnp.concatenate(
            [kv_ref[source, pl.ds(number * chunk, half), :] for number in range(rows // chunk)],
            axis=0,
        )
        lhs = jnp.concatenate([key_rows, gates[source, :, :]], axis=1)
        part = jnp.dot(lhs, rhs[side, :, :], preferred_element_type=jnp.float32)
        if limit is not None:
            row = lax.broadcasted_iota(jnp.int32, part.shape, 0)
            row = row // half * chunk + lax.rem(row, half) + side * half
            part = jnp.where(row <= limit, part, -jnp.inf)
        scores[side * (rows // 2) : (side + 1) * (rows // 2), :] = part
        return jnp.maximum(top, jnp.max(part.reshape(-1, 8, both_tiles), axis=0))

    def blend(source, scores, side, begin, top, total):
        start = side * (rows // 2) + begin * half
        weights = jnp.exp(scores[start : start + span, :] - top).astype(bf16)
        values = jnp.concatenate(
            [
                kv_ref[source, pl.ds((begin + index) * chunk + half + side * head_dim, head_dim), :]
                for index in range(span // half)
            ],
            axis=1,
        )
        return total + jnp.dot(values, weights, preferred_element_type=jnp.float32)

    def start_top():
        return jnp.full((8, both_tiles), -jnp.inf, jnp.float32)

    def settle_top(top):
        return jnp.max(top, axis=0, keepdims=True)

    def advance(old, old_scores, old_top, state, new, new_scores, limit=None):
        top = jnp.maximum(state[0], old_top)
        total = state[1] * jnp.exp(state[0] - top)
        new_top = start_top()
        for side in range(2):
            if new is not None:
                new_top = score(new, side, new_scores, new_top, limit)
            for begin in range(0, rows // chunk, span // half):
                total = blend(old, old_scores, side, begin, top, total)
        return (top, total), settle_top(new_top)

    def finish(phase, source, attended):
        scale = lax.rsqrt(jnp.mean(attended * attended, axis=0, keepdims=True) + NORM_EPSILON)
        done[phase, source, :, :] = (attended * scale * gain).astype(bf16)
        stays = jnp.logical_and(source == sp, home_here)

        @pl.when(stays)
        def _():
            stay(phase, source, slot).start()

        @pl.when(jnp.logical_not(stays))
        def _():
            away(phase, source).start()

    def attend(phase):
        def pair_of_sources(pair, _):
            even, odd = 2 * pair, 2 * pair + 1
            even_spot, odd_spot = place_here, pieces - 1 - place_here
            set_queries(phase, even, even_spot, odd, odd_spot)
            column = lax.broadcasted_iota(jnp.int32, (1, both_tiles), 1)
            inside = lax.rem(column, tile)
            inside = (inside // half * phases + phase) * half + lax.rem(inside, half)
            in_even = column < tile
            even_limit = jnp.where(in_even, inside + even_spot * piece, rows)
            odd_limit = jnp.where(in_even, -1, inside + odd_spot * piece)
            state = (
                jnp.full((1, both_tiles), -1e30, jnp.float32),
                jnp.zeros((head_dim, both_tiles), jnp.float32),
            )
            top = start_top()
            for side in range(2):
                top = score(even, side, scores_a, top, even_limit)
            state, top = advance(
                even, scores_a, settle_top(top), state, odd, scores_b, odd_limit
            )

            def two_sources(step, carried):
                state, top, last = carried
                state, top = advance(last, scores_b, top, state, 2 * step, scores_a)
                state, top = advance(2 * step, scores_a, top, state, 2 * step + 1, scores_b)
                return state, top, 2 * step + 1

            state, top, last = lax.fori_loop(0, pair, two_sources, (state, top, odd))
            state, _ = advance(last, scores_b, top, state, None, None)
            finish(phase, even, state[1][:, :tile])
            finish(phase, odd, state[1][:, tile:])
            return 0

        lax.fori_loop(0, sp_count // 2, pair_of_sources, 0)

    def arrive(phase):
        for index in range(targets * CORES):
            giver = core * targets + index // CORES
            here = jnp.logical_and(giver == sp, core == index % CORES)

            @pl.when(here)
            def _():
                stay(phase, 0, index).wait()

            @pl.when(jnp.logical_not(here))
            def _():
                mesh_copy(
                    done.at[phase, 0], landed.at[phase, index], send.at[phase, 0],
                    recv.at[phase, index], (sp, mate),
                ).wait_recv()

            head = index // (share * CORES)
            place = index % (share * CORES)
            spot = jnp.where(lax.rem(sp, 2) == 0, place, pieces - 1 - place)
            for inner in range(tile // half):
                start = pl.multiple_of((spot * slabs + inner * phases + phase) * half, half)
                flipped[head * head_dim : (head + 1) * head_dim, pl.ds(start, half)] = landed[
                    phase, index, :, inner * half : (inner + 1) * half
                ]
        for slab in range(phase, rows // half, phases):
            at = slice(slab * half, (slab + 1) * half)
            attn[at, :] = flipped[:, at].astype(jnp.float32).T.astype(bf16)

    def product(block, number):
        at = pl.ds(pl.multiple_of(block * block_rows + number * sub, sub), sub)
        return partial[at, :] + jnp.dot(
            attn[at, :], attn_weight[...], preferred_element_type=jnp.float32
        )

    def within(number):
        return pl.ds(number * sub, sub)

    def to_mate(step, number):
        at = within(number)
        return mesh_copy(
            mate_out.at[step, at], mate_in.at[step, at], mate_ssem.at[step, number],
            mate_rsem.at[step, number], (sp, mate),
        )

    def across(step, number):
        at = within(number)
        return mesh_copy(
            link_out.at[step - 1, at], link_in.at[step - 1, at], link_ssem.at[step - 1, number],
            link_rsem.at[step - 1, number], (sp, lax.rem(tp + CORES * step, tp_count)),
        )

    def joined(step, number):
        at = within(number)
        to_mate(step, number).wait_recv()
        total = keep[step, at, :] + mate_in[step, at, :].astype(jnp.float32)
        link_out[step - 1, at, :] = total.astype(jnp.bfloat16)
        across(step, number).start()

    def spread(phase):
        waiting = []
        for step in list(range(1, chips)) + [0]:
            for number in range(phase * subs, (phase + 1) * subs):
                at = within(number)
                theirs = lax.rem(mate + CORES * step, tp_count)
                ours = lax.rem(tp + CORES * step, tp_count)
                mate_out[step, at, :] = product(theirs, number).astype(jnp.bfloat16)
                to_mate(step, number).start()
                keep[step, at, :] = product(ours, number)
                if waiting:
                    joined(*waiting.pop())
                if step:
                    waiting.append((step, number))

    def settle(phase):
        for number in range(phase * subs, (phase + 1) * subs):
            at = within(number)
            to_mate(0, number).wait_recv()
            total = keep[0, at, :] + mate_in[0, at, :].astype(jnp.float32)
            for step in range(1, chips):
                across(step, number).wait_recv()
                total = total + link_in[step - 1, at, :].astype(jnp.float32)
            out_ref[at, :] = total.astype(jnp.bfloat16)

    attend(0)
    for number in range(tp_count):
        at = pl.ds(number * block_rows, block_rows)
        partial[at, :] = jnp.dot(
            conv_ref[at, :], conv_weight[...], preferred_element_type=jnp.float32
        )
    arrive(0)
    spread(0)
    for phase in range(1, phases):
        attend(phase)
        settle(phase - 1)
        arrive(phase)
        spread(phase)
    settle(phases - 1)
    for step in range(chips):
        for number in range(phases * subs):
            to_mate(step, number).wait_send()
            if step:
                across(step, number).wait_send()
    for phase in range(phases):
        for step in range(1, sp_count):
            away(phase, lax.rem(sp + step, sp_count)).wait_send()

        @pl.when(jnp.logical_not(home_here))
        def _():
            away(phase, sp).wait_send()


def rear(queries, kv, sides, conv_mixed, attn_weight, conv_weight, head_dim, piece):
    sp_count = lax.axis_size("sp")
    tp_count = lax.axis_size("tp")
    chips = tp_count // CORES
    rows, width = conv_mixed.shape
    features = attn_weight.shape[1]
    block_rows = rows // tp_count
    phases = min(2, piece // LANES)
    tile = piece // phases
    sub = min(64, block_rows // 2)
    subs = block_rows // sub
    links = max(chips - 1, 1)
    bf16 = jnp.bfloat16
    dma = pltpu.SemaphoreType.DMA
    vmem = pl.BlockSpec(memory_space=VMEM)
    return pl.pallas_call(
        functools.partial(rear_kernel, (sp_count, tp_count, head_dim, piece, sub)),
        out_shape=jax.ShapeDtypeStruct((block_rows, features), bf16),
        in_specs=[vmem] * 6,
        out_specs=vmem,
        scratch_shapes=[
            VMEM((phases, sp_count, head_dim, tile), bf16),
            VMEM((phases, sp_count, head_dim, tile), bf16),
            VMEM((2, 2 * LANES, 2 * tile), bf16),
            VMEM((sp_count, rows // 2, LANES), bf16),
            VMEM((rows, 2 * tile), jnp.float32),
            VMEM((rows, 2 * tile), jnp.float32),
            VMEM((width, rows), bf16),
            VMEM((rows, width), bf16),
            VMEM((rows, features), jnp.float32),
            VMEM((chips, block_rows, features), jnp.float32),
            VMEM((chips, block_rows, features), bf16),
            VMEM((chips, block_rows, features), bf16),
            VMEM((links, block_rows, features), bf16),
            VMEM((links, block_rows, features), bf16),
            dma((phases, sp_count)), dma((phases, sp_count)), dma((phases,)),
            dma((chips, subs)), dma((chips, subs)), dma((links, subs)), dma((links, subs)),
        ],
        compiler_params=pltpu.CompilerParams(
            collective_id=1, has_side_effects=True, vmem_limit_bytes=56 * 1024 * 1024
        ),
    )(queries, kv, sides, conv_mixed, attn_weight, conv_weight)


def per_device(
    tokens,
    mix_gain,
    query_weight,
    key_weight,
    value_weight,
    outer_gate_weight,
    inner_gate_weight,
    conv_input_weight,
    query_gain,
    key_gain,
    gate_totals,
    conv_taps,
    attn_out_gain,
    conv_out_gain,
    attn_out_weight,
    conv_out_weight,
):
    rows = tokens.shape[0]
    head_dim = query_gain.shape[0]
    width = query_weight.shape[1]
    heads = width // head_dim
    sp_count = lax.axis_size("sp")
    share = sp_count // CORES // heads
    pieces = CORES * share
    piece = rows // pieces
    gate_rows = gate_totals.T.reshape(heads, rows // LANES, LANES)
    gain_rows = jnp.pad(
        attn_out_gain.reshape(heads, 1, head_dim), ((0, 0), (0, 7), (0, LANES - head_dim))
    )
    sides = jnp.concatenate([gate_rows, gain_rows], axis=1)
    kv, queries, sides, conv_mixed = front(
        tokens,
        mix_gain.reshape(1, -1),
        query_gain.reshape(1, -1),
        key_gain.reshape(1, -1),
        conv_taps,
        conv_out_gain.reshape(1, -1),
        sides,
        (
            query_weight,
            key_weight,
            value_weight,
            outer_gate_weight,
            inner_gate_weight,
            conv_input_weight,
        ),
        head_dim,
        piece,
    )
    return rear(
        queries, kv, sides, conv_mixed, attn_out_weight, conv_out_weight, head_dim, piece
    )


def solution(mesh):
    placed = (
        P("sp", "tp"),
        P(),
        P(None, "tp"),
        P(None, "tp"),
        P(None, "tp"),
        P(None, "tp"),
        P(None, "tp"),
        P(None, "tp"),
        P(),
        P(),
        P("sp", "tp"),
        P(None, "tp"),
        P("tp"),
        P("tp"),
        P("tp", None),
        P("tp", None),
    )
    return jax.shard_map(
        per_device, mesh=mesh, in_specs=placed, out_specs=P(("sp", "tp"), None), check_vma=False
    )
```

```python
import functools

import jax
import jax.numpy as jnp
from jax import lax
from jax.experimental import pallas as pl
from jax.experimental.pallas import tpu as pltpu
from jax.sharding import PartitionSpec as P

NORM_EPSILON = 1e-06
MESH = pl.DeviceIdType.MESH
CORES = 2
LANES = 128
VMEM = pltpu.VMEM


def greet(devices):
    barrier = pltpu.get_barrier_semaphore()
    for sp, tp in devices:
        pl.semaphore_signal(barrier, inc=1, device_id=(sp, tp), device_id_type=MESH)
    pl.semaphore_wait(barrier, len(devices))


def mesh_copy(src, dst, send, recv, device):
    return pltpu.make_async_remote_copy(
        src, dst, send, recv, device_id=device, device_id_type=MESH
    )


def layer_kernel(
    plan, tokens_ref, mix_ref, query_gain_ref, key_gain_ref, taps_ref, conv_gain_ref, gates_ref,
    attn_gain_ref, *refs
):
    sp_count, tp_count, head_count, head_dim, piece, sub = plan
    weight_refs = refs[:8]
    out_ref = refs[8]
    (
        weights, attn_weight, conv_weight, gathered, scaled, row_scales, kv_send, query_send,
        side_send, outer, padded, edge_send, edge_recv, kv_in, query_in, side_in, conv_mixed,
        done, landed, rhs, gates, scores_a, scores_b, flipped, attn, partial, keep, mate_out,
        mate_in, link_out, link_in,
        weight_sem, own_sem, cross_send, mate_send, tok_pass_send, tok_recv,
        kv_ssem, kv_rsem, query_ssem, query_rsem, side_ssem, side_rsem,
        kv_psem, kv_prsem, side_psem, side_prsem, local, edge_sem,
        send, recv, stay_sem, mate_ssem, mate_rsem, link_ssem, link_rsem,
    ) = refs[9:]
    f32 = jnp.float32
    bf16 = jnp.bfloat16
    sp = lax.axis_index("sp")
    tp = lax.axis_index("tp")
    core = lax.rem(tp, CORES)
    mate = tp + 1 - 2 * core
    first = tp - core
    chips = tp_count // CORES
    targets = sp_count // CORES
    rows, features = tokens_ref.shape
    width = head_count * head_dim
    half = LANES
    chunk = 2 * half
    chunks = rows // chunk
    pieces = rows // piece
    share = pieces // CORES
    phases = min(2, piece // half)
    tile = piece // phases
    slabs = piece // half
    span = 256
    both_tiles = 2 * tile
    block_rows = rows // tp_count
    subs = block_rows // phases // sub
    order = [chunks - 1] + list(range(chunks - 1))
    home = sp // targets
    slot = lax.rem(sp, targets) * CORES + core
    owner = home == core
    place_here = lax.rem(sp, share) * CORES + core
    query_gain = jnp.concatenate([query_gain_ref[...]] * head_count, axis=1)
    key_gain = jnp.concatenate([key_gain_ref[...]] * head_count, axis=1)

    mine = pltpu.make_async_copy(tokens_ref, gathered.at[tp], own_sem)
    mine.start()
    loads = [
        pltpu.make_async_copy(
            ref, (list(weights.at[i] for i in range(6)) + [attn_weight, conv_weight])[index],
            weight_sem.at[index],
        )
        for index, ref in enumerate(weight_refs)
    ]
    for index in (1, 2, 0, 3, 4, 5, 6, 7):
        loads[index].start()
    padded[0:8, :] = jnp.zeros((8, width), f32)
    for head in range(head_count):
        lines = [
            gates_ref[head : head + 1, row * LANES : (row + 1) * LANES]
            for row in range(rows // LANES)
        ]
        gain_line = attn_gain_ref[:, head * head_dim : (head + 1) * head_dim]
        gain_line = jnp.concatenate([gain_line, jnp.zeros((1, LANES - head_dim), f32)], axis=1)
        lines.append(jnp.broadcast_to(gain_line, (8, LANES)))
        side_send[head, :, :] = jnp.concatenate(lines, axis=0)
    greet(
        [
            (lax.rem(sp + step, sp_count), first + lax.rem(core + other, CORES))
            for step in range(sp_count)
            for other in range(CORES)
            if step or other
        ]
        + [(sp, lax.rem(tp + CORES * step, tp_count)) for step in range(1, chips)]
    )

    def block(number):
        return pl.ds(number * chunk, chunk)

    def tokens_to(device, number, sem):
        return mesh_copy(
            gathered.at[tp, block(number)], gathered.at[tp, block(number)], sem,
            tok_recv.at[tp, number], device,
        )

    def to_mate_tokens(number):
        return tokens_to((sp, mate), number, mate_send.at[number])

    def across_tokens(step, number):
        return tokens_to(
            (sp, lax.rem(tp + CORES * step, tp_count)), number, cross_send.at[step - 1, number]
        )

    def token_pass(step, number):
        other = lax.rem(tp + CORES * step, tp_count)
        return mesh_copy(
            gathered.at[other, block(number)], gathered.at[other, block(number)],
            tok_pass_send.at[step - 1, number], tok_recv.at[other, number], (sp, mate),
        )

    def token_arrival(source, number):
        return mesh_copy(
            gathered.at[source, block(number)], gathered.at[source, block(number)],
            mate_send.at[number], tok_recv.at[source, number], (sp, mate),
        )

    mine.wait()
    for number in order:
        for step in range(1, chips):
            across_tokens(step, number).start()
        to_mate_tokens(number).start()

    def target_of(step):
        at = lax.rem(sp + 1 + step, targets)
        return at // share, core * targets + at

    def side_copy(step, head, target):
        return mesh_copy(
            side_send.at[head], side_in.at[sp], side_ssem.at[step], side_rsem.at[sp], (target, tp)
        )

    def kv_copy(step, number, head, target):
        return mesh_copy(
            kv_send.at[head, block(number)], kv_in.at[sp, block(number)],
            kv_ssem.at[step, number], kv_rsem.at[sp, number], (target, tp),
        )

    def kept(number, head):
        return pltpu.make_async_copy(
            kv_send.at[head, block(number)], kv_in.at[sp, block(number)], local.at[number]
        )

    def kept_side(head):
        return pltpu.make_async_copy(side_send.at[head], side_in.at[sp], local.at[chunks])

    def slab_copies(slab, starting):
        spot, inner = slab // slabs, slab % slabs
        place = jnp.where(lax.rem(sp, 2) == 0, spot, pieces - 1 - spot)
        part = pl.ds(slab * head_dim, head_dim)
        for step in range(head_count):
            head = lax.rem(sp + 1 + step, head_count)
            target = core * targets + head * share + place // CORES
            there = first + lax.rem(place, CORES)
            here = jnp.logical_and(target == sp, there == tp)

            if starting:

                @pl.when(here)
                def _():
                    pltpu.make_async_copy(
                        query_send.at[head, part], query_in.at[sp, inner],
                        query_rsem.at[sp, inner],
                    ).start()

            @pl.when(jnp.logical_not(here))
            def _():
                copy = mesh_copy(
                    query_send.at[head, part], query_in.at[sp, inner],
                    query_ssem.at[step, slab], query_rsem.at[sp, inner], (target, there),
                )
                if starting:
                    copy.start()
                else:
                    copy.wait_send()

    def query_arrival(source, inner):
        mesh_copy(
            query_send.at[0, pl.ds(0, head_dim)], query_in.at[source, inner],
            query_ssem.at[0, 0], query_rsem.at[source, inner], (sp, mate),
        ).wait_recv()

    for step in range(targets):
        head, target = target_of(step)

        @pl.when(target != sp)
        def _():
            side_copy(step, head, target).start()

        @pl.when(target == sp)
        def _():
            kept_side(head).start()

    ones_row = lax.broadcasted_iota(jnp.int32, (width, width), 0) // head_dim
    ones_column = lax.broadcasted_iota(jnp.int32, (width, width), 1) // head_dim
    spread_mean = jnp.where(ones_row == ones_column, 1.0 / head_dim, 0.0).astype(bf16)

    def normed(values, gain):
        squares = values * values
        high = squares.astype(bf16)
        low = (squares - high.astype(f32)).astype(bf16)
        mean = jnp.dot(high, spread_mean, preferred_element_type=f32)
        mean = mean + jnp.dot(low, spread_mean, preferred_element_type=f32)
        return values * lax.rsqrt(mean + NORM_EPSILON) * gain

    def project(number, index):
        product = jnp.dot(
            scaled[block(number), :], weights[index], preferred_element_type=f32
        )
        return product * row_scales[block(number), 0:1]

    def take_tokens(number):
        here = block(number)
        for step in range(1, chips):
            token_arrival(lax.rem(tp + CORES * step, tp_count), number).wait_recv()
            token_pass(step, number).start()
        token_arrival(mate, number).wait_recv()
        for step in range(1, chips):
            token_arrival(lax.rem(mate + CORES * step, tp_count), number).wait_recv()
        total = jnp.zeros((chunk, 1), f32)
        for source in range(tp_count):
            part = gathered[source, here, :].astype(f32)
            at = slice(source * features, (source + 1) * features)
            total = total + jnp.sum(part * part, axis=1, keepdims=True)
            scaled[here, at] = (part * mix_ref[:, at]).astype(bf16)
        row_scale = lax.rsqrt(total / (tp_count * features) + NORM_EPSILON)
        row_scales[here, :] = jnp.broadcast_to(row_scale, (chunk, LANES))

    def send_keys(number):
        keys = normed(project(number, 1), key_gain).astype(bf16)
        values = project(number, 2)
        for head in range(head_count):
            at = slice(head * head_dim, (head + 1) * head_dim)
            kv_send[head, pl.ds(number * chunk, half), :] = jnp.concatenate(
                [keys[:half, at], keys[half:, at]], axis=1
            )
        for side in range(2):
            rows_of = slice(side * half, (side + 1) * half)
            for lane in range(0, width, LANES):
                turned = values[rows_of, lane : lane + LANES].T.astype(bf16)
                for inner in range(LANES // head_dim):
                    kv_send[
                        lane // head_dim + inner,
                        pl.ds(number * chunk + half + side * head_dim, head_dim),
                        :,
                    ] = turned[inner * head_dim : (inner + 1) * head_dim]
        for step in range(targets):
            head, target = target_of(step)

            @pl.when(target != sp)
            def _():
                kv_copy(step, number, head, target).start()

            @pl.when(target == sp)
            def _():
                kept(number, head).start()

    def send_queries(number):
        queries = normed(project(number, 0), query_gain).astype(bf16)
        queries = queries.astype(f32) * head_dim ** (-0.5)
        for side in range(2):
            rows_of = slice(side * half, (side + 1) * half)
            for lane in range(0, width, LANES):
                turned = queries[rows_of, lane : lane + LANES].T.astype(bf16)
                for inner in range(LANES // head_dim):
                    query_send[
                        lane // head_dim + inner,
                        pl.ds(number * half + side * head_dim, head_dim),
                        :,
                    ] = turned[inner * head_dim : (inner + 1) * head_dim]
        slab_copies(2 * number, True)

    for index in (1, 2, 0):
        loads[index].wait()
    for number in order:
        take_tokens(number)
        send_keys(number)
        send_queries(number)
    for number in order:
        slab_copies(2 * number + 1, True)

    sources = [lax.rem(sp + step, sp_count) for step in range(sp_count)]

    def kv_pass(source, number):
        return mesh_copy(
            kv_in.at[source, block(number)], kv_in.at[source, block(number)],
            kv_psem.at[source, number], kv_prsem.at[source, number], (sp, mate),
        )

    def side_pass(source):
        return mesh_copy(
            side_in.at[source], side_in.at[source], side_psem.at[source], side_prsem.at[source],
            (sp, mate),
        )

    @pl.when(owner)
    def _():
        for step, source in enumerate(sources):
            if step == 0:
                kept_side(0).wait()
            else:
                mesh_copy(
                    side_send.at[0], side_in.at[source], side_ssem.at[0], side_rsem.at[source],
                    (sp, mate),
                ).wait_recv()
            side_pass(source).start()

    @pl.when(jnp.logical_not(owner))
    def _():
        for source in sources:
            side_pass(source).wait_recv()

    def forward(number):
        @pl.when(owner)
        def _():
            for step, source in enumerate(sources):
                if step == 0:
                    kept(number, 0).wait()
                else:
                    mesh_copy(
                        kv_send.at[0, block(number)], kv_in.at[source, block(number)],
                        kv_ssem.at[0, number], kv_rsem.at[source, number], (sp, mate),
                    ).wait_recv()
                kv_pass(source, number).start()

    gain_tile = jnp.broadcast_to(side_in[0, rows // LANES : rows // LANES + 1, :], (LANES, LANES))
    gain = gain_tile.T[:head_dim, 0:1]

    def pieces_of(values):
        high = values.astype(bf16).astype(f32)
        middle = (values - high).astype(bf16).astype(f32)
        low = (values - high - middle).astype(bf16).astype(f32)
        return high, middle, low

    def gate_columns(source, _):
        cuts = pieces_of(-side_in[source, : rows // LANES, :])
        for number in range(chunks):
            lines = [
                cut[2 * number + side : 2 * number + side + 1, :] for side in range(2) for cut in cuts
            ]
            lines.append(jnp.zeros((LANES - len(lines), LANES), f32))
            gates[source, number * half : (number + 1) * half, :] = (
                jnp.concatenate(lines, axis=0).T.astype(bf16)
            )
        return 0

    forward(order[0])
    lax.fori_loop(0, sp_count, gate_columns, 0)

    def conv_inputs(number):
        here = block(number)
        outer[here, :] = project(number, 3)
        gated = (project(number, 4) * project(number, 5)).astype(bf16)
        padded[pl.ds(8 + number * chunk, chunk), :] = gated.astype(f32)
        return gated

    edge = mesh_copy(
        edge_send, edge_recv, edge_sem.at[0], edge_sem.at[1], (lax.rem(sp + 1, sp_count), tp)
    )
    for index in (3, 4, 5):
        loads[index].wait()
    for position, number in enumerate(order):
        gated = conv_inputs(number)
        if position == 0:
            edge_send[...] = gated[chunk - 16 :, :]

            @pl.when(sp < sp_count - 1)
            def _():
                edge.start()

        elif position < chunks - 1:
            forward(number)

    @pl.when(sp > 0)
    def _():
        edge.wait_recv()
        padded[0:8, :] = edge_recv[8:16, :].astype(f32)

    taps = taps_ref.shape[0]
    for number in range(chunks):
        convolved = jnp.zeros((chunk, width), f32)
        for tap in range(taps):
            at = pl.ds(8 - taps + 1 + tap + number * chunk, chunk)
            convolved = convolved + taps_ref[tap : tap + 1, :] * padded[at, :]
        conv_mixed[block(number), :] = normed(
            outer[block(number), :] * convolved, conv_gain_ref[...]
        ).astype(bf16)
    loads[6].wait()
    loads[7].wait()
    for number in range(tp_count):
        at = pl.ds(number * block_rows, block_rows)
        partial[at, :] = jnp.dot(conv_mixed[at, :], conv_weight[...], preferred_element_type=f32)
    forward(order[-1])

    @pl.when(jnp.logical_not(owner))
    def _():
        for source in sources:
            for number in order:
                kv_pass(source, number).wait_recv()

    def away(phase, source):
        return mesh_copy(
            done.at[phase, source], landed.at[phase, slot], send.at[phase, source],
            recv.at[phase, slot], (source, first + home),
        )

    def stay(phase, source, index):
        return pltpu.make_async_copy(
            done.at[phase, source], landed.at[phase, index], stay_sem.at[phase]
        )

    def queries_of(phase, source):
        return jnp.concatenate(
            [query_in[source, slab, :, :] for slab in range(phase, slabs, phases)], axis=1
        )

    def set_queries(phase, even, odd):
        queries = jnp.concatenate([queries_of(phase, even), queries_of(phase, odd)], axis=1)
        empty = jnp.zeros_like(queries)
        row = lax.broadcasted_iota(jnp.int32, (LANES, both_tiles), 0)
        for side in range(2):
            ones = jnp.logical_and(row >= 3 * side, row < 3 * side + 3)
            stacked = [queries, empty] if side == 0 else [empty, queries]
            rhs[side, :, :] = jnp.concatenate(
                stacked + [jnp.where(ones, 1.0, 0.0).astype(bf16)], axis=0
            )

    def score(source, side, scores, top, limit):
        key_rows = jnp.concatenate(
            [kv_in[source, pl.ds(number * chunk, half), :] for number in range(rows // chunk)],
            axis=0,
        )
        lhs = jnp.concatenate([key_rows, gates[source, :, :]], axis=1)
        part = jnp.dot(lhs, rhs[side, :, :], preferred_element_type=f32)
        if limit is not None:
            row = lax.broadcasted_iota(jnp.int32, part.shape, 0)
            row = row // half * chunk + lax.rem(row, half) + side * half
            part = jnp.where(row <= limit, part, -jnp.inf)
        scores[side * (rows // 2) : (side + 1) * (rows // 2), :] = part
        return jnp.maximum(top, jnp.max(part.reshape(-1, 8, both_tiles), axis=0))

    def blend(source, scores, side, begin, top, total):
        start = side * (rows // 2) + begin * half
        weights = jnp.exp(scores[start : start + span, :] - top).astype(bf16)
        values = jnp.concatenate(
            [
                kv_in[source, pl.ds((begin + index) * chunk + half + side * head_dim, head_dim), :]
                for index in range(span // half)
            ],
            axis=1,
        )
        return total + jnp.dot(values, weights, preferred_element_type=f32)

    def start_top():
        return jnp.full((8, both_tiles), -jnp.inf, f32)

    def settle_top(top):
        return jnp.max(top, axis=0, keepdims=True)

    def advance(old, old_scores, old_top, state, new, new_scores, limit=None):
        top = jnp.maximum(state[0], old_top)
        total = state[1] * jnp.exp(state[0] - top)
        new_top = start_top()
        for side in range(2):
            if new is not None:
                new_top = score(new, side, new_scores, new_top, limit)
            for begin in range(0, rows // chunk, span // half):
                total = blend(old, old_scores, side, begin, top, total)
        return (top, total), settle_top(new_top)

    def finish(phase, source, attended):
        scale = lax.rsqrt(jnp.mean(attended * attended, axis=0, keepdims=True) + NORM_EPSILON)
        done[phase, source, :, :] = (attended * scale * gain).astype(bf16)
        stays = jnp.logical_and(source == sp, owner)

        @pl.when(stays)
        def _():
            stay(phase, source, slot).start()

        @pl.when(jnp.logical_not(stays))
        def _():
            away(phase, source).start()

    def attend(phase):
        for source in range(sp_count):
            for inner in range(phase, slabs, phases):
                query_arrival(source, inner)
        column = lax.broadcasted_iota(jnp.int32, (1, both_tiles), 1)
        inside = lax.rem(column, tile)
        inside = (inside // half * phases + phase) * half + lax.rem(inside, half)
        in_even = column < tile
        even_limit = jnp.where(in_even, inside + place_here * piece, rows)
        odd_limit = jnp.where(in_even, -1, inside + (pieces - 1 - place_here) * piece)
        empty = (
            jnp.full((1, both_tiles), -1e30, f32), jnp.zeros((head_dim, both_tiles), f32)
        )

        def pair_of_sources(pair, carried):
            state, top, last = carried
            even, odd = 2 * pair, 2 * pair + 1
            set_queries(phase, even, odd)
            state, top = advance(last, scores_b, top, state, even, scores_a, even_limit)

            @pl.when(pair > 0)
            def _():
                finish(phase, even - 2, state[1][:, :tile])
                finish(phase, odd - 2, state[1][:, tile:])

            state, top = advance(even, scores_a, top, empty, odd, scores_b, odd_limit)

            def two_sources(step, carried):
                state, top, last = carried
                state, top = advance(last, scores_b, top, state, 2 * step, scores_a)
                state, top = advance(2 * step, scores_a, top, state, 2 * step + 1, scores_b)
                return state, top, 2 * step + 1

            return lax.fori_loop(0, pair, two_sources, (state, top, odd))

        if phase == 0:
            scores_b[...] = jnp.zeros_like(scores_b)
        state, top, last = lax.fori_loop(
            0, sp_count // 2, pair_of_sources, (empty, jnp.zeros((1, both_tiles), f32), 0)
        )
        state, _ = advance(last, scores_b, top, state, None, None)
        finish(phase, sp_count - 2, state[1][:, :tile])
        finish(phase, sp_count - 1, state[1][:, tile:])

    def arrive(phase):
        for index in range(targets * CORES):
            giver = core * targets + index // CORES
            here = jnp.logical_and(giver == sp, core == index % CORES)

            @pl.when(here)
            def _():
                stay(phase, 0, index).wait()

            @pl.when(jnp.logical_not(here))
            def _():
                mesh_copy(
                    done.at[phase, 0], landed.at[phase, index], send.at[phase, 0],
                    recv.at[phase, index], (sp, mate),
                ).wait_recv()

            head = index // (share * CORES)
            place = index % (share * CORES)
            spot = jnp.where(lax.rem(sp, 2) == 0, place, pieces - 1 - place)
            for inner in range(tile // half):
                start = pl.multiple_of((spot * slabs + inner * phases + phase) * half, half)
                flipped[head * head_dim : (head + 1) * head_dim, pl.ds(start, half)] = landed[
                    phase, index, :, inner * half : (inner + 1) * half
                ]
        for slab in range(phase, rows // half, phases):
            at = slice(slab * half, (slab + 1) * half)
            attn[at, :] = flipped[:, at].astype(f32).T.astype(bf16)

    def product(block, number):
        at = pl.ds(pl.multiple_of(block * block_rows + number * sub, sub), sub)
        return partial[at, :] + jnp.dot(
            attn[at, :], attn_weight[...], preferred_element_type=f32
        )

    def within(number):
        return pl.ds(number * sub, sub)

    def to_mate(step, number):
        at = within(number)
        return mesh_copy(
            mate_out.at[step, at], mate_in.at[step, at], mate_ssem.at[step, number],
            mate_rsem.at[step, number], (sp, mate),
        )

    def across(step, number):
        at = within(number)
        return mesh_copy(
            link_out.at[step - 1, at], link_in.at[step - 1, at], link_ssem.at[step - 1, number],
            link_rsem.at[step - 1, number], (sp, lax.rem(tp + CORES * step, tp_count)),
        )

    def joined(step, number):
        at = within(number)
        to_mate(step, number).wait_recv()
        total = keep[step, at, :] + mate_in[step, at, :].astype(f32)
        link_out[step - 1, at, :] = total.astype(bf16)
        across(step, number).start()

    def spread(phase):
        waiting = []
        for step in list(range(1, chips)) + [0]:
            for number in range(phase * subs, (phase + 1) * subs):
                at = within(number)
                theirs = lax.rem(mate + CORES * step, tp_count)
                ours = lax.rem(tp + CORES * step, tp_count)
                mate_out[step, at, :] = product(theirs, number).astype(bf16)
                to_mate(step, number).start()
                keep[step, at, :] = product(ours, number)
                if waiting:
                    joined(*waiting.pop())
                if step:
                    waiting.append((step, number))

    def settle(phase):
        for number in range(phase * subs, (phase + 1) * subs):
            at = within(number)
            to_mate(0, number).wait_recv()
            total = keep[0, at, :] + mate_in[0, at, :].astype(f32)
            for step in range(1, chips):
                across(step, number).wait_recv()
                total = total + link_in[step - 1, at, :].astype(f32)
            out_ref[at, :] = total.astype(bf16)

    attend(0)
    arrive(0)
    spread(0)
    for phase in range(1, phases):
        attend(phase)
        settle(phase - 1)
        arrive(phase)
        spread(phase)
    settle(phases - 1)
    for step in range(chips):
        for number in range(phases * subs):
            to_mate(step, number).wait_send()
            if step:
                across(step, number).wait_send()
    for phase in range(phases):
        for step in range(1, sp_count):
            away(phase, lax.rem(sp + step, sp_count)).wait_send()

        @pl.when(jnp.logical_not(owner))
        def _():
            away(phase, sp).wait_send()

    @pl.when(owner)
    def _():
        for source in sources:
            side_pass(source).wait_send()
            for number in order:
                kv_pass(source, number).wait_send()

    for step in range(targets):
        head, target = target_of(step)

        @pl.when(target != sp)
        def _():
            side_copy(step, head, target).wait_send()
            for number in order:
                kv_copy(step, number, head, target).wait_send()

    for slab in range(2 * chunks):
        slab_copies(slab, False)
    for number in order:
        to_mate_tokens(number).wait_send()
        for step in range(1, chips):
            across_tokens(step, number).wait_send()
            token_pass(step, number).wait_send()

    @pl.when(sp < sp_count - 1)
    def _():
        edge.wait_send()


def layer(
    tokens, mix_gain, query_gain, key_gain, taps, conv_gain, gate_rows, attn_gain, weights, head_dim
):
    sp_count = lax.axis_size("sp")
    tp_count = lax.axis_size("tp")
    rows, features = tokens.shape
    width = weights[0].shape[1]
    out_features = weights[6].shape[1]
    heads = width // head_dim
    pieces = sp_count // heads
    piece = rows // pieces
    phases = min(2, piece // LANES)
    tile = piece // phases
    slabs = piece // LANES
    chunks = rows // LANES // 2
    chips = tp_count // CORES
    targets = sp_count // CORES
    block_rows = rows // tp_count
    sub = min(64, block_rows // 2)
    subs = block_rows // sub
    links = max(chips - 1, 1)
    bf16 = jnp.bfloat16
    f32 = jnp.float32
    dma = pltpu.SemaphoreType.DMA
    vmem = pl.BlockSpec(memory_space=VMEM)
    hbm = pl.BlockSpec(memory_space=pl.ANY)
    return pl.pallas_call(
        functools.partial(layer_kernel, (sp_count, tp_count, heads, head_dim, piece, sub)),
        out_shape=jax.ShapeDtypeStruct((block_rows, out_features), bf16),
        in_specs=[hbm] + [vmem] * 7 + [hbm] * 8,
        out_specs=vmem,
        scratch_shapes=[
            VMEM((6,) + weights[0].shape, bf16),
            VMEM(weights[6].shape, bf16),
            VMEM(weights[7].shape, bf16),
            VMEM((tp_count, rows, features), bf16),
            VMEM((rows, tp_count * features), bf16),
            VMEM((rows, LANES), f32),
            VMEM((heads, rows, LANES), bf16),
            VMEM((heads, rows // 2, LANES), bf16),
            VMEM((heads, rows // LANES + 8, LANES), f32),
            VMEM((rows, width), f32),
            VMEM((rows + 8, width), f32),
            VMEM((16, width), bf16),
            VMEM((16, width), bf16),
            VMEM((sp_count, rows, LANES), bf16),
            VMEM((sp_count, slabs, head_dim, LANES), bf16),
            VMEM((sp_count, rows // LANES + 8, LANES), f32),
            VMEM((rows, width), bf16),
            VMEM((phases, sp_count, head_dim, tile), bf16),
            VMEM((phases, sp_count, head_dim, tile), bf16),
            VMEM((2, 2 * LANES, 2 * tile), bf16),
            VMEM((sp_count, rows // 2, LANES), bf16),
            VMEM((rows, 2 * tile), f32),
            VMEM((rows, 2 * tile), f32),
            VMEM((width, rows), bf16),
            VMEM((rows, width), bf16),
            VMEM((rows, out_features), f32),
            VMEM((chips, block_rows, out_features), f32),
            VMEM((chips, block_rows, out_features), bf16),
            VMEM((chips, block_rows, out_features), bf16),
            VMEM((links, block_rows, out_features), bf16),
            VMEM((links, block_rows, out_features), bf16),
            dma((8,)), dma, dma((links, chunks)), dma((chunks,)), dma((links, chunks)),
            dma((tp_count, chunks)),
            dma((targets, chunks)), dma((sp_count, chunks)),
            dma((heads, 2 * chunks)), dma((sp_count, slabs)),
            dma((targets,)), dma((sp_count,)),
            dma((sp_count, chunks)), dma((sp_count, chunks)),
            dma((sp_count,)), dma((sp_count,)),
            dma((chunks + 1,)), dma((2,)),
            dma((phases, sp_count)), dma((phases, sp_count)), dma((phases,)),
            dma((chips, subs)), dma((chips, subs)), dma((links, subs)), dma((links, subs)),
        ],
        compiler_params=pltpu.CompilerParams(
            collective_id=0, has_side_effects=True, vmem_limit_bytes=63 * 1024 * 1024
        ),
    )(tokens, mix_gain, query_gain, key_gain, taps, conv_gain, gate_rows, attn_gain, *weights)


def per_device(
    tokens,
    mix_gain,
    query_weight,
    key_weight,
    value_weight,
    outer_gate_weight,
    inner_gate_weight,
    conv_input_weight,
    query_gain,
    key_gain,
    gate_totals,
    conv_taps,
    attn_out_gain,
    conv_out_gain,
    attn_out_weight,
    conv_out_weight,
):
    return layer(
        tokens,
        mix_gain.reshape(1, -1),
        query_gain.reshape(1, -1),
        key_gain.reshape(1, -1),
        conv_taps,
        conv_out_gain.reshape(1, -1),
        gate_totals.T,
        attn_out_gain.reshape(1, -1),
        (
            query_weight,
            key_weight,
            value_weight,
            outer_gate_weight,
            inner_gate_weight,
            conv_input_weight,
            attn_out_weight,
            conv_out_weight,
        ),
        query_gain.shape[0],
    )


def solution(mesh):
    placed = (
        P("sp", "tp"),
        P(),
        P(None, "tp"),
        P(None, "tp"),
        P(None, "tp"),
        P(None, "tp"),
        P(None, "tp"),
        P(None, "tp"),
        P(),
        P(),
        P("sp", "tp"),
        P(None, "tp"),
        P("tp"),
        P("tp"),
        P("tp", None),
        P("tp", None),
    )
    return jax.shard_map(
        per_device, mesh=mesh, in_specs=placed, out_specs=P(("sp", "tp"), None), check_vma=False
    )
```

```python
import functools

import jax
import jax.numpy as jnp
from jax import lax
from jax.experimental import pallas as pl
from jax.experimental.pallas import tpu as pltpu
from jax.sharding import PartitionSpec as P

NORM_EPSILON = 1e-06
MESH = pl.DeviceIdType.MESH
CORES = 2
LANES = 128
VMEM = pltpu.VMEM


def greet(devices):
    barrier = pltpu.get_barrier_semaphore()
    for sp, tp in devices:
        pl.semaphore_signal(barrier, inc=1, device_id=(sp, tp), device_id_type=MESH)
    pl.semaphore_wait(barrier, len(devices))


def mesh_copy(src, dst, send, recv, device):
    return pltpu.make_async_remote_copy(
        src, dst, send, recv, device_id=device, device_id_type=MESH
    )


def layer_kernel(
    plan, tokens_ref, mix_ref, query_gain_ref, key_gain_ref, taps_ref, conv_gain_ref, gates_ref,
    attn_gain_ref, *refs
):
    sp_count, tp_count, head_count, head_dim, piece = plan
    weight_refs = refs[:8]
    out_ref = refs[8]
    (
        weights, out_weights, gathered, scaled, row_scales, kv_send, query_send,
        side_send, outer, padded, edge_send, edge_recv, kv_in, query_in, side_in, conv_mixed,
        conv_in, done, landed, rhs, gates, scores_a, scores_b, conv_rows,
        weight_sem, own_sem, cross_send, mate_send, tok_pass_send, tok_recv,
        kv_ssem, kv_rsem, query_ssem, query_rsem, side_ssem, side_rsem,
        kv_psem, kv_prsem, side_psem, side_prsem, local, edge_sem,
        send, recv, conv_ssem, conv_rsem, out_recv, out_cross, out_side, out_mate,
    ) = refs[9:]
    f32 = jnp.float32
    bf16 = jnp.bfloat16
    sp = lax.axis_index("sp")
    tp = lax.axis_index("tp")
    core = lax.rem(tp, CORES)
    mate = tp + 1 - 2 * core
    first = tp - core
    chips = tp_count // CORES
    targets = sp_count // CORES
    rows, features = tokens_ref.shape
    width = head_count * head_dim
    half = LANES
    chunk = 2 * half
    chunks = rows // chunk
    pieces = rows // piece
    share = pieces // CORES
    phases = min(2, piece // half)
    tile = piece // phases
    slabs = piece // half
    span = 256
    both_tiles = 2 * tile
    block_rows = rows // tp_count
    parts = 4
    part_rows = width // parts
    parity = lax.rem(sp, 2)
    beside = sp + 1 - 2 * parity
    order = [chunks - 1] + list(range(chunks - 1))
    home = sp // targets
    head_slot = (first + home) * head_count + lax.rem(sp, targets) // share
    owner = home == core
    place_here = lax.rem(sp, share) * CORES + core
    query_gain = jnp.concatenate([query_gain_ref[...]] * head_count, axis=1)
    key_gain = jnp.concatenate([key_gain_ref[...]] * head_count, axis=1)

    mine = pltpu.make_async_copy(tokens_ref, gathered.at[tp], own_sem)
    mine.start()
    loads = [
        pltpu.make_async_copy(
            ref,
            weights.at[index]
            if index < 6
            else out_weights.at[index - 6, pl.ds(pl.multiple_of(tp * width, width), width)],
            weight_sem.at[index],
        )
        for index, ref in enumerate(weight_refs)
    ]
    for index in (1, 2, 0, 3, 4, 5, 6, 7):
        loads[index].start()
    padded[0:8, :] = jnp.zeros((8, width), f32)
    for head in range(head_count):
        lines = [
            gates_ref[head : head + 1, row * LANES : (row + 1) * LANES]
            for row in range(rows // LANES)
        ]
        gain_line = attn_gain_ref[:, head * head_dim : (head + 1) * head_dim]
        gain_line = jnp.concatenate([gain_line, jnp.zeros((1, LANES - head_dim), f32)], axis=1)
        lines.append(jnp.broadcast_to(gain_line, (8, LANES)))
        side_send[head, :, :] = jnp.concatenate(lines, axis=0)
    greet(
        [
            (lax.rem(sp + step, sp_count), lax.rem(tp + other, tp_count))
            for step in range(sp_count)
            for other in range(tp_count)
            if step or other
        ]
    )

    def block(number):
        return pl.ds(number * chunk, chunk)

    def tokens_to(device, number, sem):
        return mesh_copy(
            gathered.at[tp, block(number)], gathered.at[tp, block(number)], sem,
            tok_recv.at[tp, number], device,
        )

    def to_mate_tokens(number):
        return tokens_to((sp, mate), number, mate_send.at[number])

    def across_tokens(step, number):
        return tokens_to(
            (sp, lax.rem(tp + CORES * step, tp_count)), number, cross_send.at[step - 1, number]
        )

    def token_pass(step, number):
        other = lax.rem(tp + CORES * step, tp_count)
        return mesh_copy(
            gathered.at[other, block(number)], gathered.at[other, block(number)],
            tok_pass_send.at[step - 1, number], tok_recv.at[other, number], (sp, mate),
        )

    def token_arrival(source, number):
        return mesh_copy(
            gathered.at[source, block(number)], gathered.at[source, block(number)],
            mate_send.at[number], tok_recv.at[source, number], (sp, mate),
        )

    mine.wait()
    for number in order:
        for step in range(1, chips):
            across_tokens(step, number).start()
        to_mate_tokens(number).start()

    def target_of(step):
        at = lax.rem(sp + 1 + step, targets)
        return at // share, core * targets + at

    def side_copy(step, head, target):
        return mesh_copy(
            side_send.at[head], side_in.at[sp], side_ssem.at[step], side_rsem.at[sp], (target, tp)
        )

    def kv_copy(step, number, head, target):
        return mesh_copy(
            kv_send.at[head, block(number)], kv_in.at[sp, block(number)],
            kv_ssem.at[step, number], kv_rsem.at[sp, number], (target, tp),
        )

    def kept(number, head):
        return pltpu.make_async_copy(
            kv_send.at[head, block(number)], kv_in.at[sp, block(number)], local.at[number]
        )

    def kept_side(head):
        return pltpu.make_async_copy(side_send.at[head], side_in.at[sp], local.at[chunks])

    def slab_copies(slab, starting):
        spot, inner = slab // slabs, slab % slabs
        place = jnp.where(lax.rem(sp, 2) == 0, spot, pieces - 1 - spot)
        part = pl.ds(slab * head_dim, head_dim)
        for step in range(head_count):
            head = lax.rem(sp + 1 + step, head_count)
            target = core * targets + head * share + place // CORES
            there = first + lax.rem(place, CORES)
            here = jnp.logical_and(target == sp, there == tp)

            if starting:

                @pl.when(here)
                def _():
                    pltpu.make_async_copy(
                        query_send.at[head, part], query_in.at[sp, inner],
                        query_rsem.at[sp, inner],
                    ).start()

            @pl.when(jnp.logical_not(here))
            def _():
                copy = mesh_copy(
                    query_send.at[head, part], query_in.at[sp, inner],
                    query_ssem.at[step, slab], query_rsem.at[sp, inner], (target, there),
                )
                if starting:
                    copy.start()
                else:
                    copy.wait_send()

    def query_arrival(source, inner):
        mesh_copy(
            query_send.at[0, pl.ds(0, head_dim)], query_in.at[source, inner],
            query_ssem.at[0, 0], query_rsem.at[source, inner], (sp, mate),
        ).wait_recv()

    for step in range(targets):
        head, target = target_of(step)

        @pl.when(target != sp)
        def _():
            side_copy(step, head, target).start()

        @pl.when(target == sp)
        def _():
            kept_side(head).start()

    ones_row = lax.broadcasted_iota(jnp.int32, (width, width), 0) // head_dim
    ones_column = lax.broadcasted_iota(jnp.int32, (width, width), 1) // head_dim
    spread_mean = jnp.where(ones_row == ones_column, 1.0 / head_dim, 0.0).astype(bf16)

    def normed(values, gain):
        squares = values * values
        high = squares.astype(bf16)
        low = (squares - high.astype(f32)).astype(bf16)
        mean = jnp.dot(high, spread_mean, preferred_element_type=f32)
        mean = mean + jnp.dot(low, spread_mean, preferred_element_type=f32)
        return values * lax.rsqrt(mean + NORM_EPSILON) * gain

    def project(number, index):
        product = jnp.dot(
            scaled[block(number), :], weights[index], preferred_element_type=f32
        )
        return product * row_scales[block(number), 0:1]

    def take_tokens(number):
        here = block(number)
        for step in range(1, chips):
            token_arrival(lax.rem(tp + CORES * step, tp_count), number).wait_recv()
            token_pass(step, number).start()
        token_arrival(mate, number).wait_recv()
        for step in range(1, chips):
            token_arrival(lax.rem(mate + CORES * step, tp_count), number).wait_recv()
        total = jnp.zeros((chunk, 1), f32)
        for source in range(tp_count):
            part = gathered[source, here, :].astype(f32)
            at = slice(source * features, (source + 1) * features)
            total = total + jnp.sum(part * part, axis=1, keepdims=True)
            scaled[here, at] = (part * mix_ref[:, at]).astype(bf16)
        row_scale = lax.rsqrt(total / (tp_count * features) + NORM_EPSILON)
        row_scales[here, :] = jnp.broadcast_to(row_scale, (chunk, LANES))

    def send_keys(number):
        keys = normed(project(number, 1), key_gain).astype(bf16)
        values = project(number, 2)
        for head in range(head_count):
            at = slice(head * head_dim, (head + 1) * head_dim)
            kv_send[head, pl.ds(number * chunk, half), :] = jnp.concatenate(
                [keys[:half, at], keys[half:, at]], axis=1
            )
        for side in range(2):
            rows_of = slice(side * half, (side + 1) * half)
            for lane in range(0, width, LANES):
                turned = values[rows_of, lane : lane + LANES].T.astype(bf16)
                for inner in range(LANES // head_dim):
                    kv_send[
                        lane // head_dim + inner,
                        pl.ds(number * chunk + half + side * head_dim, head_dim),
                        :,
                    ] = turned[inner * head_dim : (inner + 1) * head_dim]
        for step in range(targets):
            head, target = target_of(step)

            @pl.when(target != sp)
            def _():
                kv_copy(step, number, head, target).start()

            @pl.when(target == sp)
            def _():
                kept(number, head).start()

    def send_queries(number):
        queries = normed(project(number, 0), query_gain).astype(bf16)
        queries = queries.astype(f32) * head_dim ** (-0.5)
        for side in range(2):
            rows_of = slice(side * half, (side + 1) * half)
            for lane in range(0, width, LANES):
                turned = queries[rows_of, lane : lane + LANES].T.astype(bf16)
                for inner in range(LANES // head_dim):
                    query_send[
                        lane // head_dim + inner,
                        pl.ds(number * half + side * head_dim, head_dim),
                        :,
                    ] = turned[inner * head_dim : (inner + 1) * head_dim]
        slab_copies(2 * number, True)

    for index in (1, 2, 0):
        loads[index].wait()
    for number in order:
        take_tokens(number)
        send_keys(number)
        send_queries(number)
    for number in order:
        slab_copies(2 * number + 1, True)

    def part_of(kind, source, part):
        at = pl.multiple_of(source * width + part * part_rows, part_rows)
        return out_weights.at[kind, pl.ds(at, part_rows)]

    def weights_to(kind, source, part, sem, device):
        ref = part_of(kind, source, part)
        return mesh_copy(ref, ref, sem, out_recv.at[kind, source, part], device)

    def weights_across(step, part):
        return weights_to(
            parity, tp, part, out_cross.at[step - 1, part],
            (sp, lax.rem(tp + CORES * step, tp_count)),
        )

    def weights_beside(step, part):
        source = lax.rem(tp + CORES * step, tp_count)
        return weights_to(parity, source, part, out_side.at[step - 1, part], (beside, tp))

    def weights_mate(kind, source, part):
        return weights_to(kind, source, part, out_mate.at[kind, source, part], (sp, mate))

    def from_across(part):
        for step in range(1, chips):
            source = lax.rem(tp + CORES * step, tp_count)
            weights_mate(parity, source, part).wait_recv()
            weights_beside(step, part).start()
            weights_mate(parity, source, part).start()

    def from_beside(part):
        for step in range(1, chips):
            source = lax.rem(tp + CORES * step, tp_count)
            weights_mate(1 - parity, source, part).wait_recv()
            weights_mate(1 - parity, source, part).start()

    loads[6].wait()
    loads[7].wait()
    for step in range(1, chips):
        for number in order:
            across_tokens(step, number).wait_send()
        for part in range(parts):
            weights_across(step, part).start()

    sources = [lax.rem(sp + step, sp_count) for step in range(sp_count)]

    def kv_pass(source, number):
        return mesh_copy(
            kv_in.at[source, block(number)], kv_in.at[source, block(number)],
            kv_psem.at[source, number], kv_prsem.at[source, number], (sp, mate),
        )

    def side_pass(source):
        return mesh_copy(
            side_in.at[source], side_in.at[source], side_psem.at[source], side_prsem.at[source],
            (sp, mate),
        )

    @pl.when(owner)
    def _():
        for step, source in enumerate(sources):
            if step == 0:
                kept_side(0).wait()
            else:
                mesh_copy(
                    side_send.at[0], side_in.at[source], side_ssem.at[0], side_rsem.at[source],
                    (sp, mate),
                ).wait_recv()
            side_pass(source).start()

    @pl.when(jnp.logical_not(owner))
    def _():
        for source in sources:
            side_pass(source).wait_recv()

    def forward(number):
        @pl.when(owner)
        def _():
            for step, source in enumerate(sources):
                if step == 0:
                    kept(number, 0).wait()
                else:
                    mesh_copy(
                        kv_send.at[0, block(number)], kv_in.at[source, block(number)],
                        kv_ssem.at[0, number], kv_rsem.at[source, number], (sp, mate),
                    ).wait_recv()
                kv_pass(source, number).start()

    gain_tile = jnp.broadcast_to(side_in[0, rows // LANES : rows // LANES + 1, :], (LANES, LANES))
    gain = gain_tile.T[:head_dim, 0:1]

    def pieces_of(values):
        high = values.astype(bf16).astype(f32)
        middle = (values - high).astype(bf16).astype(f32)
        low = (values - high - middle).astype(bf16).astype(f32)
        return high, middle, low

    def gate_columns(source, _):
        cuts = pieces_of(-side_in[source, : rows // LANES, :])
        for number in range(chunks):
            lines = [
                cut[2 * number + side : 2 * number + side + 1, :] for side in range(2) for cut in cuts
            ]
            lines.append(jnp.zeros((LANES - len(lines), LANES), f32))
            gates[source, number * half : (number + 1) * half, :] = (
                jnp.concatenate(lines, axis=0).T.astype(bf16)
            )
        return 0

    forward(order[0])
    lax.fori_loop(0, sp_count, gate_columns, 0)

    def conv_inputs(number):
        here = block(number)
        outer[here, :] = project(number, 3)
        gated = (project(number, 4) * project(number, 5)).astype(bf16)
        padded[pl.ds(8 + number * chunk, chunk), :] = gated.astype(f32)
        return gated

    edge = mesh_copy(
        edge_send, edge_recv, edge_sem.at[0], edge_sem.at[1], (lax.rem(sp + 1, sp_count), tp)
    )
    for index in (3, 4, 5):
        loads[index].wait()
    for position, number in enumerate(order):
        gated = conv_inputs(number)
        if position == 0:
            edge_send[...] = gated[chunk - 16 :, :]

            @pl.when(sp < sp_count - 1)
            def _():
                edge.start()

        elif position < chunks - 1:
            forward(number)

    @pl.when(sp > 0)
    def _():
        edge.wait_recv()
        padded[0:8, :] = edge_recv[8:16, :].astype(f32)

    taps = taps_ref.shape[0]
    for number in range(chunks):
        convolved = jnp.zeros((chunk, width), f32)
        for tap in range(taps):
            at = pl.ds(8 - taps + 1 + tap + number * chunk, chunk)
            convolved = convolved + taps_ref[tap : tap + 1, :] * padded[at, :]
        conv_mixed[block(number), :] = normed(
            outer[block(number), :] * convolved, conv_gain_ref[...]
        ).astype(bf16)

    def conv_share(step):
        there = lax.rem(tp + step, tp_count)
        at = pl.ds(pl.multiple_of(there * block_rows, block_rows), block_rows)
        return mesh_copy(
            conv_mixed.at[at], conv_in.at[tp], conv_ssem.at[step - 1], conv_rsem.at[tp],
            (sp, there),
        )

    for step in range(1, tp_count):
        conv_share(step).start()
    own_rows = pl.ds(pl.multiple_of(tp * block_rows, block_rows), block_rows)
    conv_in[tp, :, :] = conv_mixed[own_rows, :]
    forward(order[-1])

    @pl.when(jnp.logical_not(owner))
    def _():
        for source in sources:
            for number in order:
                kv_pass(source, number).wait_recv()

    for kind in range(2):
        for part in range(parts):
            weights_mate(kind, tp, part).start()
    for part in range(parts // 2):
        from_across(part)

    def place_of(phase, inner, spot):
        begin = (inner * phases + phase) * half
        return spot * (piece // block_rows) + begin // block_rows, begin % block_rows

    def away(phase, source, inner, spot):
        there, at = place_of(phase, inner, spot)
        return mesh_copy(
            done.at[phase, source, :, pl.ds(inner * half, half)],
            landed.at[head_slot, :, pl.ds(at, half)],
            send.at[phase, source, inner], recv.at[head_slot, at // half], (source, there),
        )

    def stays_here(phase, source, inner, spot):
        return jnp.logical_and(source == sp, place_of(phase, inner, spot)[0] == tp)

    even_spot, odd_spot = place_here, pieces - 1 - place_here

    def queries_of(phase, source):
        return jnp.concatenate(
            [query_in[source, slab, :, :] for slab in range(phase, slabs, phases)], axis=1
        )

    def set_queries(phase, even, odd):
        queries = jnp.concatenate([queries_of(phase, even), queries_of(phase, odd)], axis=1)
        empty = jnp.zeros_like(queries)
        row = lax.broadcasted_iota(jnp.int32, (LANES, both_tiles), 0)
        for side in range(2):
            ones = jnp.logical_and(row >= 3 * side, row < 3 * side + 3)
            stacked = [queries, empty] if side == 0 else [empty, queries]
            rhs[side, :, :] = jnp.concatenate(
                stacked + [jnp.where(ones, 1.0, 0.0).astype(bf16)], axis=0
            )

    def score(source, side, scores, top, limit):
        key_rows = jnp.concatenate(
            [kv_in[source, pl.ds(number * chunk, half), :] for number in range(rows // chunk)],
            axis=0,
        )
        lhs = jnp.concatenate([key_rows, gates[source, :, :]], axis=1)
        part = jnp.dot(lhs, rhs[side, :, :], preferred_element_type=f32)
        if limit is not None:
            row = lax.broadcasted_iota(jnp.int32, part.shape, 0)
            row = row // half * chunk + lax.rem(row, half) + side * half
            part = jnp.where(row <= limit, part, -jnp.inf)
        scores[side * (rows // 2) : (side + 1) * (rows // 2), :] = part
        return jnp.maximum(top, jnp.max(part.reshape(-1, 8, both_tiles), axis=0))

    def blend(source, scores, side, begin, top, total):
        start = side * (rows // 2) + begin * half
        weights = jnp.exp(scores[start : start + span, :] - top).astype(bf16)
        values = jnp.concatenate(
            [
                kv_in[source, pl.ds((begin + index) * chunk + half + side * head_dim, head_dim), :]
                for index in range(span // half)
            ],
            axis=1,
        )
        return total + jnp.dot(values, weights, preferred_element_type=f32)

    def start_top():
        return jnp.full((8, both_tiles), -jnp.inf, f32)

    def settle_top(top):
        return jnp.max(top, axis=0, keepdims=True)

    def advance(old, old_scores, old_top, state, new, new_scores, limit=None):
        top = jnp.maximum(state[0], old_top)
        total = state[1] * jnp.exp(state[0] - top)
        new_top = start_top()
        for side in range(2):
            if new is not None:
                new_top = score(new, side, new_scores, new_top, limit)
            for begin in range(0, rows // chunk, span // half):
                total = blend(old, old_scores, side, begin, top, total)
        return (top, total), settle_top(new_top)

    def finish(phase, source, attended, spot):
        scale = lax.rsqrt(jnp.mean(attended * attended, axis=0, keepdims=True) + NORM_EPSILON)
        done[phase, source, :, :] = (attended * scale * gain).astype(bf16)
        for inner in range(tile // half):
            stays = stays_here(phase, source, inner, spot)

            @pl.when(stays)
            def _():
                at = place_of(phase, inner, spot)[1]
                pltpu.make_async_copy(
                    done.at[phase, source, :, pl.ds(inner * half, half)],
                    landed.at[head_slot, :, pl.ds(at, half)],
                    recv.at[head_slot, at // half],
                ).start()

            @pl.when(jnp.logical_not(stays))
            def _():
                away(phase, source, inner, spot).start()

    def attend(phase):
        for source in range(sp_count):
            for inner in range(phase, slabs, phases):
                query_arrival(source, inner)
        column = lax.broadcasted_iota(jnp.int32, (1, both_tiles), 1)
        inside = lax.rem(column, tile)
        inside = (inside // half * phases + phase) * half + lax.rem(inside, half)
        in_even = column < tile
        even_limit = jnp.where(in_even, inside + even_spot * piece, rows)
        odd_limit = jnp.where(in_even, -1, inside + odd_spot * piece)
        empty = (
            jnp.full((1, both_tiles), -1e30, f32), jnp.zeros((head_dim, both_tiles), f32)
        )

        def pair_of_sources(pair, carried):
            state, top, last = carried
            even, odd = 2 * pair, 2 * pair + 1
            set_queries(phase, even, odd)
            state, top = advance(last, scores_b, top, state, even, scores_a, even_limit)

            @pl.when(pair > 0)
            def _():
                finish(phase, even - 2, state[1][:, :tile], even_spot)
                finish(phase, odd - 2, state[1][:, tile:], odd_spot)

            state, top = advance(even, scores_a, top, empty, odd, scores_b, odd_limit)

            def two_sources(step, carried):
                state, top, last = carried
                state, top = advance(last, scores_b, top, state, 2 * step, scores_a)
                state, top = advance(2 * step, scores_a, top, state, 2 * step + 1, scores_b)
                return state, top, 2 * step + 1

            return lax.fori_loop(0, pair, two_sources, (state, top, odd))

        if phase == 0:
            scores_b[...] = jnp.zeros_like(scores_b)
        state, top, last = lax.fori_loop(
            0, sp_count // 2, pair_of_sources, (empty, jnp.zeros((1, both_tiles), f32), 0)
        )
        state, _ = advance(last, scores_b, top, state, None, None)
        finish(phase, sp_count - 2, state[1][:, :tile], even_spot)
        finish(phase, sp_count - 1, state[1][:, tile:], odd_spot)

    for phase in range(phases):
        attend(phase)
        if phase == 0:
            for part in range(parts // 2, parts):
                from_across(part)
    for part in range(parts):
        from_beside(part)
    for step in range(1, tp_count):
        source = lax.rem(tp + step, tp_count)
        mesh_copy(
            conv_mixed.at[pl.ds(0, block_rows)], conv_in.at[source], conv_ssem.at[0],
            conv_rsem.at[source], (sp, mate),
        ).wait_recv()
    for step in range(chips):
        source = lax.rem(mate + CORES * step, tp_count)
        for kind in range(2):
            for part in range(parts):
                weights_mate(kind, source, part).wait_recv()
    out_span = 512
    out_features = out_ref.shape[1]
    conv_rows_in = jnp.concatenate([conv_in[source, :, :] for source in range(tp_count)], axis=1)
    for begin in range(0, out_features, out_span):
        at = slice(begin, begin + out_span)
        conv_rows[:, at] = jnp.dot(
            conv_rows_in, out_weights[1, :, at], preferred_element_type=f32
        )
    for phase in range(phases):
        for index in range(phase, block_rows // half, phases):
            for source in range(tp_count * head_count):
                mesh_copy(
                    done.at[0, 0, :, pl.ds(0, half)],
                    landed.at[source, :, pl.ds(index * half, half)],
                    send.at[0, 0, 0], recv.at[source, index], (sp, mate),
                ).wait_recv()
            here = slice(index * half, (index + 1) * half)
            mixed = landed[:, :, here].reshape(tp_count * width, half)
            mixed = mixed.astype(f32).T.astype(bf16)
            for begin in range(0, out_features, out_span):
                at = slice(begin, begin + out_span)
                out_ref[here, at] = (
                    conv_rows[here, at]
                    + jnp.dot(mixed, out_weights[0, :, at], preferred_element_type=f32)
                ).astype(bf16)
    for phase in range(phases):
        for source in range(sp_count):
            for inner in range(tile // half):
                spot = odd_spot if source % 2 else even_spot

                @pl.when(jnp.logical_not(stays_here(phase, source, inner, spot)))
                def _():
                    away(phase, source, inner, spot).wait_send()

    for step in range(1, tp_count):
        conv_share(step).wait_send()
    for part in range(parts):
        for kind in range(2):
            for step in range(chips):
                weights_mate(kind, lax.rem(tp + CORES * step, tp_count), part).wait_send()
        for step in range(1, chips):
            weights_across(step, part).wait_send()
            weights_beside(step, part).wait_send()

    @pl.when(owner)
    def _():
        for source in sources:
            side_pass(source).wait_send()
            for number in order:
                kv_pass(source, number).wait_send()

    for step in range(targets):
        head, target = target_of(step)

        @pl.when(target != sp)
        def _():
            side_copy(step, head, target).wait_send()
            for number in order:
                kv_copy(step, number, head, target).wait_send()

    for slab in range(2 * chunks):
        slab_copies(slab, False)
    for number in order:
        to_mate_tokens(number).wait_send()
        for step in range(1, chips):
            token_pass(step, number).wait_send()

    @pl.when(sp < sp_count - 1)
    def _():
        edge.wait_send()


def layer(
    tokens, mix_gain, query_gain, key_gain, taps, conv_gain, gate_rows, attn_gain, weights, head_dim
):
    sp_count = lax.axis_size("sp")
    tp_count = lax.axis_size("tp")
    rows, features = tokens.shape
    width = weights[0].shape[1]
    out_features = weights[6].shape[1]
    heads = width // head_dim
    pieces = sp_count // heads
    piece = rows // pieces
    phases = min(2, piece // LANES)
    tile = piece // phases
    slabs = piece // LANES
    chunks = rows // LANES // 2
    chips = tp_count // CORES
    targets = sp_count // CORES
    block_rows = rows // tp_count
    parts = 4
    links = max(chips - 1, 1)
    bf16 = jnp.bfloat16
    f32 = jnp.float32
    dma = pltpu.SemaphoreType.DMA
    vmem = pl.BlockSpec(memory_space=VMEM)
    hbm = pl.BlockSpec(memory_space=pl.ANY)
    return pl.pallas_call(
        functools.partial(layer_kernel, (sp_count, tp_count, heads, head_dim, piece)),
        out_shape=jax.ShapeDtypeStruct((block_rows, out_features), bf16),
        in_specs=[hbm] + [vmem] * 7 + [hbm] * 8,
        out_specs=vmem,
        scratch_shapes=[
            VMEM((6,) + weights[0].shape, bf16),
            VMEM((2, tp_count * width, out_features), bf16),
            VMEM((tp_count, rows, features), bf16),
            VMEM((rows, tp_count * features), bf16),
            VMEM((rows, LANES), f32),
            VMEM((heads, rows, LANES), bf16),
            VMEM((heads, rows // 2, LANES), bf16),
            VMEM((heads, rows // LANES + 8, LANES), f32),
            VMEM((rows, width), f32),
            VMEM((rows + 8, width), f32),
            VMEM((16, width), bf16),
            VMEM((16, width), bf16),
            VMEM((sp_count, rows, LANES), bf16),
            VMEM((sp_count, slabs, head_dim, LANES), bf16),
            VMEM((sp_count, rows // LANES + 8, LANES), f32),
            VMEM((rows, width), bf16),
            VMEM((tp_count, block_rows, width), bf16),
            VMEM((phases, sp_count, head_dim, tile), bf16),
            VMEM((tp_count * heads, head_dim, block_rows), bf16),
            VMEM((2, 2 * LANES, 2 * tile), bf16),
            VMEM((sp_count, rows // 2, LANES), bf16),
            VMEM((rows, 2 * tile), f32),
            VMEM((rows, 2 * tile), f32),
            VMEM((block_rows, out_features), f32),
            dma((8,)), dma, dma((links, chunks)), dma((chunks,)), dma((links, chunks)),
            dma((tp_count, chunks)),
            dma((targets, chunks)), dma((sp_count, chunks)),
            dma((heads, 2 * chunks)), dma((sp_count, slabs)),
            dma((targets,)), dma((sp_count,)),
            dma((sp_count, chunks)), dma((sp_count, chunks)),
            dma((sp_count,)), dma((sp_count,)),
            dma((chunks + 1,)), dma((2,)),
            dma((phases, sp_count, tile // LANES)), dma((tp_count * heads, block_rows // LANES)),
            dma((tp_count - 1,)), dma((tp_count,)),
            dma((2, tp_count, parts)), dma((links, parts)), dma((links, parts)),
            dma((2, tp_count, parts)),
        ],
        compiler_params=pltpu.CompilerParams(
            collective_id=0, has_side_effects=True, vmem_limit_bytes=63 * 1024 * 1024
        ),
    )(tokens, mix_gain, query_gain, key_gain, taps, conv_gain, gate_rows, attn_gain, *weights)


def per_device(
    tokens,
    mix_gain,
    query_weight,
    key_weight,
    value_weight,
    outer_gate_weight,
    inner_gate_weight,
    conv_input_weight,
    query_gain,
    key_gain,
    gate_totals,
    conv_taps,
    attn_out_gain,
    conv_out_gain,
    attn_out_weight,
    conv_out_weight,
):
    return layer(
        tokens,
        mix_gain.reshape(1, -1),
        query_gain.reshape(1, -1),
        key_gain.reshape(1, -1),
        conv_taps,
        conv_out_gain.reshape(1, -1),
        gate_totals.T,
        attn_out_gain.reshape(1, -1),
        (
            query_weight,
            key_weight,
            value_weight,
            outer_gate_weight,
            inner_gate_weight,
            conv_input_weight,
            attn_out_weight,
            conv_out_weight,
        ),
        query_gain.shape[0],
    )


def solution(mesh):
    placed = (
        P("sp", "tp"),
        P(),
        P(None, "tp"),
        P(None, "tp"),
        P(None, "tp"),
        P(None, "tp"),
        P(None, "tp"),
        P(None, "tp"),
        P(),
        P(),
        P("sp", "tp"),
        P(None, "tp"),
        P("tp"),
        P("tp"),
        P("tp", None),
        P("tp", None),
    )
    return jax.shard_map(
        per_device, mesh=mesh, in_specs=placed, out_specs=P(("sp", "tp"), None), check_vma=False
    )
```

```python
import functools

import jax
import jax.numpy as jnp
from jax import lax
from jax.experimental import pallas as pl
from jax.experimental.pallas import tpu as pltpu
from jax.sharding import PartitionSpec as P

NORM_EPSILON = 1e-06
MESH = pl.DeviceIdType.MESH
CORES = 2
LANES = 128
VMEM = pltpu.VMEM


def greet(devices):
    barrier = pltpu.get_barrier_semaphore()
    for sp, tp in devices:
        pl.semaphore_signal(barrier, inc=1, device_id=(sp, tp), device_id_type=MESH)
    pl.semaphore_wait(barrier, len(devices))


def mesh_copy(src, dst, send, recv, device):
    return pltpu.make_async_remote_copy(
        src, dst, send, recv, device_id=device, device_id_type=MESH
    )


def layer_kernel(
    plan, tokens_ref, mix_ref, query_gain_ref, key_gain_ref, taps_ref, conv_gain_ref, gates_ref,
    attn_gain_ref, *refs
):
    sp_count, tp_count, head_count, head_dim, piece = plan
    weight_refs = refs[:8]
    out_ref = refs[8]
    (
        weights, out_weights, gathered, scaled, row_scales, kv_send, query_send,
        side_send, outer, padded, edge_send, edge_recv, kv_in, query_in, side_in, conv_mixed,
        conv_in, done, landed, rhs, gates, scores_a, scores_b, conv_rows,
        weight_sem, own_sem, cross_send, mate_send, tok_pass_send, tok_recv,
        kv_ssem, kv_rsem, query_ssem, query_rsem, side_ssem, side_rsem,
        kv_psem, kv_prsem, side_psem, side_prsem, local, edge_sem,
        send, recv, conv_ssem, conv_rsem, out_recv, out_cross, out_side, out_mate,
    ) = refs[9:]
    f32 = jnp.float32
    bf16 = jnp.bfloat16
    sp = lax.axis_index("sp")
    tp = lax.axis_index("tp")
    core = lax.rem(tp, CORES)
    mate = tp + 1 - 2 * core
    first = tp - core
    chips = tp_count // CORES
    targets = sp_count // CORES
    rows, features = tokens_ref.shape
    width = head_count * head_dim
    half = LANES
    chunk = 2 * half
    chunks = rows // chunk
    pieces = rows // piece
    share = pieces // CORES
    phases = min(2, piece // half)
    tile = piece // phases
    slabs = piece // half
    span = 256
    both_tiles = 2 * tile
    block_rows = rows // tp_count
    parts = 4
    part_rows = width // parts
    parity = lax.rem(sp, 2)
    beside = sp + 1 - 2 * parity
    order = [chunks - 1] + list(range(chunks - 1))
    home = sp // targets
    head_slot = (first + home) * head_count + lax.rem(sp, targets) // share
    owner = home == core
    place_here = lax.rem(sp, share) * CORES + core
    query_gain = jnp.concatenate([query_gain_ref[...]] * head_count, axis=1)
    key_gain = jnp.concatenate([key_gain_ref[...]] * head_count, axis=1)

    mine = pltpu.make_async_copy(tokens_ref, gathered.at[tp], own_sem)
    mine.start()
    loads = [
        pltpu.make_async_copy(
            ref,
            weights.at[index]
            if index < 6
            else out_weights.at[index - 6, pl.ds(pl.multiple_of(tp * width, width), width)],
            weight_sem.at[index],
        )
        for index, ref in enumerate(weight_refs)
    ]
    for index in (1, 2, 0, 3, 4, 5, 6, 7):
        loads[index].start()
    padded[0:8, :] = jnp.zeros((8, width), f32)
    for head in range(head_count):
        lines = [
            gates_ref[head : head + 1, row * LANES : (row + 1) * LANES]
            for row in range(rows // LANES)
        ]
        gain_line = attn_gain_ref[:, head * head_dim : (head + 1) * head_dim]
        gain_line = jnp.concatenate([gain_line, jnp.zeros((1, LANES - head_dim), f32)], axis=1)
        lines.append(jnp.broadcast_to(gain_line, (8, LANES)))
        side_send[head, :, :] = jnp.concatenate(lines, axis=0)
    greet(
        [
            (lax.rem(sp + step, sp_count), lax.rem(tp + other, tp_count))
            for step in range(sp_count)
            for other in range(tp_count)
            if step or other
        ]
    )

    def block(number):
        return pl.ds(number * chunk, chunk)

    def tokens_to(device, number, sem):
        return mesh_copy(
            gathered.at[tp, block(number)], gathered.at[tp, block(number)], sem,
            tok_recv.at[tp, number], device,
        )

    def to_mate_tokens(number):
        return tokens_to((sp, mate), number, mate_send.at[number])

    def across_tokens(step, number):
        return tokens_to(
            (sp, lax.rem(tp + CORES * step, tp_count)), number, cross_send.at[step - 1, number]
        )

    def token_pass(step, number):
        other = lax.rem(tp + CORES * step, tp_count)
        return mesh_copy(
            gathered.at[other, block(number)], gathered.at[other, block(number)],
            tok_pass_send.at[step - 1, number], tok_recv.at[other, number], (sp, mate),
        )

    def token_arrival(source, number):
        return mesh_copy(
            gathered.at[source, block(number)], gathered.at[source, block(number)],
            mate_send.at[number], tok_recv.at[source, number], (sp, mate),
        )

    mine.wait()
    for number in order:
        for step in range(1, chips):
            across_tokens(step, number).start()
        to_mate_tokens(number).start()

    def target_of(step):
        at = lax.rem(sp + 1 + step, targets)
        return at // share, core * targets + at

    def side_copy(step, head, target):
        return mesh_copy(
            side_send.at[head], side_in.at[sp], side_ssem.at[step], side_rsem.at[sp], (target, tp)
        )

    def kv_copy(step, number, head, target):
        return mesh_copy(
            kv_send.at[head, block(number)], kv_in.at[sp, block(number)],
            kv_ssem.at[step, number], kv_rsem.at[sp, number], (target, tp),
        )

    def kept(number, head):
        return pltpu.make_async_copy(
            kv_send.at[head, block(number)], kv_in.at[sp, block(number)], local.at[number]
        )

    def kept_side(head):
        return pltpu.make_async_copy(side_send.at[head], side_in.at[sp], local.at[chunks])

    def slab_copies(slab, starting):
        spot, inner = slab // slabs, slab % slabs
        place = jnp.where(lax.rem(sp, 2) == 0, spot, pieces - 1 - spot)
        part = pl.ds(slab * head_dim, head_dim)
        for step in range(head_count):
            head = lax.rem(sp + 1 + step, head_count)
            target = core * targets + head * share + place // CORES
            there = first + lax.rem(place, CORES)
            here = jnp.logical_and(target == sp, there == tp)

            if starting:

                @pl.when(here)
                def _():
                    pltpu.make_async_copy(
                        query_send.at[head, part], query_in.at[sp, inner],
                        query_rsem.at[sp, inner],
                    ).start()

            @pl.when(jnp.logical_not(here))
            def _():
                copy = mesh_copy(
                    query_send.at[head, part], query_in.at[sp, inner],
                    query_ssem.at[step, slab], query_rsem.at[sp, inner], (target, there),
                )
                if starting:
                    copy.start()
                else:
                    copy.wait_send()

    def query_arrival(source, inner):
        mesh_copy(
            query_send.at[0, pl.ds(0, head_dim)], query_in.at[source, inner],
            query_ssem.at[0, 0], query_rsem.at[source, inner], (sp, mate),
        ).wait_recv()

    for step in range(targets):
        head, target = target_of(step)

        @pl.when(target != sp)
        def _():
            side_copy(step, head, target).start()

        @pl.when(target == sp)
        def _():
            kept_side(head).start()

    ones_row = lax.broadcasted_iota(jnp.int32, (width, width), 0) // head_dim
    ones_column = lax.broadcasted_iota(jnp.int32, (width, width), 1) // head_dim
    spread_mean = jnp.where(ones_row == ones_column, 1.0 / head_dim, 0.0).astype(bf16)

    def normed(values, gain):
        squares = values * values
        high = squares.astype(bf16)
        low = (squares - high.astype(f32)).astype(bf16)
        mean = jnp.dot(high, spread_mean, preferred_element_type=f32)
        mean = mean + jnp.dot(low, spread_mean, preferred_element_type=f32)
        return values * lax.rsqrt(mean + NORM_EPSILON) * gain

    def project(number, index):
        product = jnp.dot(
            scaled[block(number), :], weights[index], preferred_element_type=f32
        )
        return product * row_scales[block(number), 0:1]

    def take_tokens(number):
        here = block(number)
        for step in range(1, chips):
            token_arrival(lax.rem(tp + CORES * step, tp_count), number).wait_recv()
            token_pass(step, number).start()
        token_arrival(mate, number).wait_recv()
        for step in range(1, chips):
            token_arrival(lax.rem(mate + CORES * step, tp_count), number).wait_recv()
        total = jnp.zeros((chunk, 1), f32)
        for source in range(tp_count):
            part = gathered[source, here, :].astype(f32)
            at = slice(source * features, (source + 1) * features)
            total = total + jnp.sum(part * part, axis=1, keepdims=True)
            scaled[here, at] = (part * mix_ref[:, at]).astype(bf16)
        row_scale = lax.rsqrt(total / (tp_count * features) + NORM_EPSILON)
        row_scales[here, :] = jnp.broadcast_to(row_scale, (chunk, LANES))

    def send_keys(number):
        keys = normed(project(number, 1), key_gain).astype(bf16)
        values = project(number, 2)
        for head in range(head_count):
            at = slice(head * head_dim, (head + 1) * head_dim)
            kv_send[head, pl.ds(number * chunk, half), :] = jnp.concatenate(
                [keys[:half, at], keys[half:, at]], axis=1
            )
        for side in range(2):
            rows_of = slice(side * half, (side + 1) * half)
            for lane in range(0, width, LANES):
                turned = values[rows_of, lane : lane + LANES].T.astype(bf16)
                for inner in range(LANES // head_dim):
                    kv_send[
                        lane // head_dim + inner,
                        pl.ds(number * chunk + half + side * head_dim, head_dim),
                        :,
                    ] = turned[inner * head_dim : (inner + 1) * head_dim]
        for step in range(targets):
            head, target = target_of(step)

            @pl.when(target != sp)
            def _():
                kv_copy(step, number, head, target).start()

            @pl.when(target == sp)
            def _():
                kept(number, head).start()

    def send_queries(number):
        queries = normed(project(number, 0), query_gain).astype(bf16)
        queries = queries.astype(f32) * head_dim ** (-0.5)
        for side in range(2):
            rows_of = slice(side * half, (side + 1) * half)
            for lane in range(0, width, LANES):
                turned = queries[rows_of, lane : lane + LANES].T.astype(bf16)
                for inner in range(LANES // head_dim):
                    query_send[
                        lane // head_dim + inner,
                        pl.ds(number * half + side * head_dim, head_dim),
                        :,
                    ] = turned[inner * head_dim : (inner + 1) * head_dim]
        slab_copies(2 * number, True)

    def part_of(kind, source, part):
        at = pl.multiple_of(source * width + part * part_rows, part_rows)
        return out_weights.at[kind, pl.ds(at, part_rows)]

    def weights_to(kind, source, part, sem, device):
        ref = part_of(kind, source, part)
        return mesh_copy(ref, ref, sem, out_recv.at[kind, source, part], device)

    def weights_across(step, part):
        return weights_to(
            parity, tp, part, out_cross.at[step - 1, part],
            (sp, lax.rem(tp + CORES * step, tp_count)),
        )

    def weights_last(step):
        return weights_to(
            1 - parity, tp, parts - 1, out_cross.at[step - 1, parts],
            (sp, lax.rem(tp + CORES * step, tp_count)),
        )

    def weights_beside(step, part):
        source = lax.rem(tp + CORES * step, tp_count)
        return weights_to(parity, source, part, out_side.at[step - 1, part], (beside, tp))

    def weights_mate(kind, source, part):
        return weights_to(kind, source, part, out_mate.at[kind, source, part], (sp, mate))

    def from_across(part):
        for step in range(1, chips):
            source = lax.rem(tp + CORES * step, tp_count)
            weights_mate(parity, source, part).wait_recv()
            if part < parts - 1:
                weights_beside(step, part).start()
            weights_mate(parity, source, part).start()

    def from_beside(part):
        for step in range(1, chips):
            source = lax.rem(tp + CORES * step, tp_count)
            weights_mate(1 - parity, source, part).wait_recv()
            weights_mate(1 - parity, source, part).start()

    def start_weights():
        loads[6].wait()
        loads[7].wait()
        for step in range(1, chips):
            for number in order:
                across_tokens(step, number).wait_send()
            for part in range(parts):
                weights_across(step, part).start()
            weights_last(step).start()

    sources = [lax.rem(sp + step, sp_count) for step in range(sp_count)]

    def kv_pass(source, number):
        return mesh_copy(
            kv_in.at[source, block(number)], kv_in.at[source, block(number)],
            kv_psem.at[source, number], kv_prsem.at[source, number], (sp, mate),
        )

    def side_pass(source):
        return mesh_copy(
            side_in.at[source], side_in.at[source], side_psem.at[source], side_prsem.at[source],
            (sp, mate),
        )

    def forward(number):
        @pl.when(owner)
        def _():
            for step, source in enumerate(sources):
                if step == 0:
                    kept(number, 0).wait()
                else:
                    mesh_copy(
                        kv_send.at[0, block(number)], kv_in.at[source, block(number)],
                        kv_ssem.at[0, number], kv_rsem.at[source, number], (sp, mate),
                    ).wait_recv()
                kv_pass(source, number).start()

    def pieces_of(values):
        high = values.astype(bf16).astype(f32)
        middle = (values - high).astype(bf16).astype(f32)
        low = (values - high - middle).astype(bf16).astype(f32)
        return high, middle, low

    def gate_columns(source, _):
        cuts = pieces_of(-side_in[source, : rows // LANES, :])
        for number in range(chunks):
            lines = [
                cut[2 * number + side : 2 * number + side + 1, :] for side in range(2) for cut in cuts
            ]
            lines.append(jnp.zeros((LANES - len(lines), LANES), f32))
            gates[source, number * half : (number + 1) * half, :] = (
                jnp.concatenate(lines, axis=0).T.astype(bf16)
            )
        return 0

    def conv_inputs(number):
        here = block(number)
        outer[here, :] = project(number, 3)
        gated = (project(number, 4) * project(number, 5)).astype(bf16)
        padded[pl.ds(8 + number * chunk, chunk), :] = gated.astype(f32)
        return gated

    edge = mesh_copy(
        edge_send, edge_recv, edge_sem.at[0], edge_sem.at[1], (lax.rem(sp + 1, sp_count), tp)
    )
    def take_sides():
        @pl.when(owner)
        def _():
            for step, source in enumerate(sources):
                if step == 0:
                    kept_side(0).wait()
                else:
                    mesh_copy(
                        side_send.at[0], side_in.at[source], side_ssem.at[0], side_rsem.at[source],
                        (sp, mate),
                    ).wait_recv()
                side_pass(source).start()

        @pl.when(jnp.logical_not(owner))
        def _():
            for source in sources:
                side_pass(source).wait_recv()

        lax.fori_loop(0, sp_count, gate_columns, 0)

    for index in (1, 2, 0, 3, 4, 5):
        loads[index].wait()
    for position, number in enumerate(order):
        take_tokens(number)
        send_keys(number)
        send_queries(number)
        if position == chunks - 1:
            for other in order:
                slab_copies(2 * other + 1, True)
            start_weights()
        gated = conv_inputs(number)
        if position == 0:
            edge_send[...] = gated[chunk - 16 :, :]

            @pl.when(sp < sp_count - 1)
            def _():
                edge.start()

            take_sides()
        if position > 1:
            forward(order[position - 2])
    gain_tile = jnp.broadcast_to(side_in[0, rows // LANES : rows // LANES + 1, :], (LANES, LANES))
    gain = gain_tile.T[:head_dim, 0:1]


    @pl.when(sp > 0)
    def _():
        edge.wait_recv()
        padded[0:8, :] = edge_recv[8:16, :].astype(f32)

    taps = taps_ref.shape[0]
    for number in range(chunks):
        convolved = jnp.zeros((chunk, width), f32)
        for tap in range(taps):
            at = pl.ds(8 - taps + 1 + tap + number * chunk, chunk)
            convolved = convolved + taps_ref[tap : tap + 1, :] * padded[at, :]
        conv_mixed[block(number), :] = normed(
            outer[block(number), :] * convolved, conv_gain_ref[...]
        ).astype(bf16)

    def conv_share(step):
        there = lax.rem(tp + step, tp_count)
        at = pl.ds(pl.multiple_of(there * block_rows, block_rows), block_rows)
        return mesh_copy(
            conv_mixed.at[at], conv_in.at[tp], conv_ssem.at[step - 1], conv_rsem.at[tp],
            (sp, there),
        )

    for step in range(1, tp_count):
        conv_share(step).start()
    own_rows = pl.ds(pl.multiple_of(tp * block_rows, block_rows), block_rows)
    conv_in[tp, :, :] = conv_mixed[own_rows, :]
    forward(order[-2])
    from_across(0)
    forward(order[-1])
    from_across(1)

    @pl.when(jnp.logical_not(owner))
    def _():
        for source in sources:
            for number in order:
                kv_pass(source, number).wait_recv()

    for kind in range(2):
        for part in range(parts):
            weights_mate(kind, tp, part).start()

    def place_of(phase, inner, spot):
        begin = (inner * phases + phase) * half
        return spot * (piece // block_rows) + begin // block_rows, begin % block_rows

    def away(phase, source, inner, spot):
        there, at = place_of(phase, inner, spot)
        return mesh_copy(
            done.at[phase, source, :, pl.ds(inner * half, half)],
            landed.at[head_slot, :, pl.ds(at, half)],
            send.at[phase, source, inner], recv.at[head_slot, at // half], (source, there),
        )

    def stays_here(phase, source, inner, spot):
        return jnp.logical_and(source == sp, place_of(phase, inner, spot)[0] == tp)

    even_spot, odd_spot = place_here, pieces - 1 - place_here

    def queries_of(phase, source):
        return jnp.concatenate(
            [query_in[source, slab, :, :] for slab in range(phase, slabs, phases)], axis=1
        )

    def set_queries(phase, even, odd):
        queries = jnp.concatenate([queries_of(phase, even), queries_of(phase, odd)], axis=1)
        empty = jnp.zeros_like(queries)
        row = lax.broadcasted_iota(jnp.int32, (LANES, both_tiles), 0)
        for side in range(2):
            ones = jnp.logical_and(row >= 3 * side, row < 3 * side + 3)
            stacked = [queries, empty] if side == 0 else [empty, queries]
            rhs[side, :, :] = jnp.concatenate(
                stacked + [jnp.where(ones, 1.0, 0.0).astype(bf16)], axis=0
            )

    def score(source, side, scores, top, limit):
        key_rows = jnp.concatenate(
            [kv_in[source, pl.ds(number * chunk, half), :] for number in range(rows // chunk)],
            axis=0,
        )
        lhs = jnp.concatenate([key_rows, gates[source, :, :]], axis=1)
        part = jnp.dot(lhs, rhs[side, :, :], preferred_element_type=f32)
        if limit is not None:
            row = lax.broadcasted_iota(jnp.int32, part.shape, 0)
            row = row // half * chunk + lax.rem(row, half) + side * half
            part = jnp.where(row <= limit, part, -jnp.inf)
        scores[side * (rows // 2) : (side + 1) * (rows // 2), :] = part
        return jnp.maximum(top, jnp.max(part.reshape(-1, 8, both_tiles), axis=0))

    def blend(source, scores, side, begin, top, total):
        start = side * (rows // 2) + begin * half
        weights = jnp.exp(scores[start : start + span, :] - top).astype(bf16)
        values = jnp.concatenate(
            [
                kv_in[source, pl.ds((begin + index) * chunk + half + side * head_dim, head_dim), :]
                for index in range(span // half)
            ],
            axis=1,
        )
        return total + jnp.dot(values, weights, preferred_element_type=f32)

    def start_top():
        return jnp.full((8, both_tiles), -jnp.inf, f32)

    def settle_top(top):
        return jnp.max(top, axis=0, keepdims=True)

    def advance(old, old_scores, old_top, state, new, new_scores, limit=None):
        top = jnp.maximum(state[0], old_top)
        total = state[1] * jnp.exp(state[0] - top)
        new_top = start_top()
        for side in range(2):
            if new is not None:
                new_top = score(new, side, new_scores, new_top, limit)
            for begin in range(0, rows // chunk, span // half):
                total = blend(old, old_scores, side, begin, top, total)
        return (top, total), settle_top(new_top)

    def finish(phase, source, attended, spot):
        scale = lax.rsqrt(jnp.mean(attended * attended, axis=0, keepdims=True) + NORM_EPSILON)
        done[phase, source, :, :] = (attended * scale * gain).astype(bf16)
        for inner in range(tile // half):
            stays = stays_here(phase, source, inner, spot)

            @pl.when(stays)
            def _():
                at = place_of(phase, inner, spot)[1]
                pltpu.make_async_copy(
                    done.at[phase, source, :, pl.ds(inner * half, half)],
                    landed.at[head_slot, :, pl.ds(at, half)],
                    recv.at[head_slot, at // half],
                ).start()

            @pl.when(jnp.logical_not(stays))
            def _():
                away(phase, source, inner, spot).start()

    def attend(phase):
        for source in range(sp_count):
            for inner in range(phase, slabs, phases):
                query_arrival(source, inner)
        column = lax.broadcasted_iota(jnp.int32, (1, both_tiles), 1)
        inside = lax.rem(column, tile)
        inside = (inside // half * phases + phase) * half + lax.rem(inside, half)
        in_even = column < tile
        even_limit = jnp.where(in_even, inside + even_spot * piece, rows)
        odd_limit = jnp.where(in_even, -1, inside + odd_spot * piece)
        empty = (
            jnp.full((1, both_tiles), -1e30, f32), jnp.zeros((head_dim, both_tiles), f32)
        )

        def pair_of_sources(pair, carried):
            state, top, last = carried
            even, odd = 2 * pair, 2 * pair + 1
            set_queries(phase, even, odd)
            state, top = advance(last, scores_b, top, state, even, scores_a, even_limit)

            @pl.when(pair > 0)
            def _():
                finish(phase, even - 2, state[1][:, :tile], even_spot)
                finish(phase, odd - 2, state[1][:, tile:], odd_spot)

            state, top = advance(even, scores_a, top, empty, odd, scores_b, odd_limit)

            def two_sources(step, carried):
                state, top, last = carried
                state, top = advance(last, scores_b, top, state, 2 * step, scores_a)
                state, top = advance(2 * step, scores_a, top, state, 2 * step + 1, scores_b)
                return state, top, 2 * step + 1

            return lax.fori_loop(0, pair, two_sources, (state, top, odd))

        if phase == 0:
            scores_b[...] = jnp.zeros_like(scores_b)
        carried = (empty, jnp.zeros((1, both_tiles), f32), 0)
        pairs = sp_count // 2
        carried = lax.fori_loop(0, pairs - 1, pair_of_sources, carried)
        hook(phase)
        state, top, last = lax.fori_loop(pairs - 1, pairs, pair_of_sources, carried)
        state, _ = advance(last, scores_b, top, state, None, None)
        finish(phase, sp_count - 2, state[1][:, :tile], even_spot)
        finish(phase, sp_count - 1, state[1][:, tile:], odd_spot)

    def hook(phase):
        if phase == 0:
            from_across(2)
            from_across(3)
        if phase == phases - 1:
            for part in range(parts):
                from_beside(part)

    for phase in range(phases):
        attend(phase)
    for step in range(1, tp_count):
        source = lax.rem(tp + step, tp_count)
        mesh_copy(
            conv_mixed.at[pl.ds(0, block_rows)], conv_in.at[source], conv_ssem.at[0],
            conv_rsem.at[source], (sp, mate),
        ).wait_recv()
    for step in range(chips):
        source = lax.rem(mate + CORES * step, tp_count)
        for kind in range(2):
            for part in range(parts):
                weights_mate(kind, source, part).wait_recv()
    out_span = 512
    out_features = out_ref.shape[1]
    conv_rows_in = jnp.concatenate([conv_in[source, :, :] for source in range(tp_count)], axis=1)
    for begin in range(0, out_features, out_span):
        at = slice(begin, begin + out_span)
        conv_rows[:, at] = jnp.dot(
            conv_rows_in, out_weights[1, :, at], preferred_element_type=f32
        )
    for phase in range(phases):
        for index in range(phase, block_rows // half, phases):
            for source in range(tp_count * head_count):
                mesh_copy(
                    done.at[0, 0, :, pl.ds(0, half)],
                    landed.at[source, :, pl.ds(index * half, half)],
                    send.at[0, 0, 0], recv.at[source, index], (sp, mate),
                ).wait_recv()
            here = slice(index * half, (index + 1) * half)
            mixed = landed[:, :, here].reshape(tp_count * width, half)
            mixed = mixed.astype(f32).T.astype(bf16)
            for begin in range(0, out_features, out_span):
                at = slice(begin, begin + out_span)
                out_ref[here, at] = (
                    conv_rows[here, at]
                    + jnp.dot(mixed, out_weights[0, :, at], preferred_element_type=f32)
                ).astype(bf16)
    for phase in range(phases):
        for source in range(sp_count):
            for inner in range(tile // half):
                spot = odd_spot if source % 2 else even_spot

                @pl.when(jnp.logical_not(stays_here(phase, source, inner, spot)))
                def _():
                    away(phase, source, inner, spot).wait_send()

    for step in range(1, tp_count):
        conv_share(step).wait_send()
    for part in range(parts):
        for kind in range(2):
            for step in range(chips):
                weights_mate(kind, lax.rem(tp + CORES * step, tp_count), part).wait_send()
        for step in range(1, chips):
            weights_across(step, part).wait_send()
            if part < parts - 1:
                weights_beside(step, part).wait_send()
            else:
                weights_last(step).wait_send()

    @pl.when(owner)
    def _():
        for source in sources:
            side_pass(source).wait_send()
            for number in order:
                kv_pass(source, number).wait_send()

    for step in range(targets):
        head, target = target_of(step)

        @pl.when(target != sp)
        def _():
            side_copy(step, head, target).wait_send()
            for number in order:
                kv_copy(step, number, head, target).wait_send()

    for slab in range(2 * chunks):
        slab_copies(slab, False)
    for number in order:
        to_mate_tokens(number).wait_send()
        for step in range(1, chips):
            token_pass(step, number).wait_send()

    @pl.when(sp < sp_count - 1)
    def _():
        edge.wait_send()


def layer(
    tokens, mix_gain, query_gain, key_gain, taps, conv_gain, gate_rows, attn_gain, weights, head_dim
):
    sp_count = lax.axis_size("sp")
    tp_count = lax.axis_size("tp")
    rows, features = tokens.shape
    width = weights[0].shape[1]
    out_features = weights[6].shape[1]
    heads = width // head_dim
    pieces = sp_count // heads
    piece = rows // pieces
    phases = min(2, piece // LANES)
    tile = piece // phases
    slabs = piece // LANES
    chunks = rows // LANES // 2
    chips = tp_count // CORES
    targets = sp_count // CORES
    block_rows = rows // tp_count
    parts = 4
    links = max(chips - 1, 1)
    bf16 = jnp.bfloat16
    f32 = jnp.float32
    dma = pltpu.SemaphoreType.DMA
    vmem = pl.BlockSpec(memory_space=VMEM)
    hbm = pl.BlockSpec(memory_space=pl.ANY)
    return pl.pallas_call(
        functools.partial(layer_kernel, (sp_count, tp_count, heads, head_dim, piece)),
        out_shape=jax.ShapeDtypeStruct((block_rows, out_features), bf16),
        in_specs=[hbm] + [vmem] * 7 + [hbm] * 8,
        out_specs=vmem,
        scratch_shapes=[
            VMEM((6,) + weights[0].shape, bf16),
            VMEM((2, tp_count * width, out_features), bf16),
            VMEM((tp_count, rows, features), bf16),
            VMEM((rows, tp_count * features), bf16),
            VMEM((rows, LANES), f32),
            VMEM((heads, rows, LANES), bf16),
            VMEM((heads, rows // 2, LANES), bf16),
            VMEM((heads, rows // LANES + 8, LANES), f32),
            VMEM((rows, width), f32),
            VMEM((rows + 8, width), f32),
            VMEM((16, width), bf16),
            VMEM((16, width), bf16),
            VMEM((sp_count, rows, LANES), bf16),
            VMEM((sp_count, slabs, head_dim, LANES), bf16),
            VMEM((sp_count, rows // LANES + 8, LANES), f32),
            VMEM((rows, width), bf16),
            VMEM((tp_count, block_rows, width), bf16),
            VMEM((phases, sp_count, head_dim, tile), bf16),
            VMEM((tp_count * heads, head_dim, block_rows), bf16),
            VMEM((2, 2 * LANES, 2 * tile), bf16),
            VMEM((sp_count, rows // 2, LANES), bf16),
            VMEM((rows, 2 * tile), f32),
            VMEM((rows, 2 * tile), f32),
            VMEM((block_rows, out_features), f32),
            dma((8,)), dma, dma((links, chunks)), dma((chunks,)), dma((links, chunks)),
            dma((tp_count, chunks)),
            dma((targets, chunks)), dma((sp_count, chunks)),
            dma((heads, 2 * chunks)), dma((sp_count, slabs)),
            dma((targets,)), dma((sp_count,)),
            dma((sp_count, chunks)), dma((sp_count, chunks)),
            dma((sp_count,)), dma((sp_count,)),
            dma((chunks + 1,)), dma((2,)),
            dma((phases, sp_count, tile // LANES)), dma((tp_count * heads, block_rows // LANES)),
            dma((tp_count - 1,)), dma((tp_count,)),
            dma((2, tp_count, parts)), dma((links, parts + 1)), dma((links, parts)),
            dma((2, tp_count, parts)),
        ],
        compiler_params=pltpu.CompilerParams(
            collective_id=0, has_side_effects=True, vmem_limit_bytes=63 * 1024 * 1024
        ),
    )(tokens, mix_gain, query_gain, key_gain, taps, conv_gain, gate_rows, attn_gain, *weights)


def per_device(
    tokens,
    mix_gain,
    query_weight,
    key_weight,
    value_weight,
    outer_gate_weight,
    inner_gate_weight,
    conv_input_weight,
    query_gain,
    key_gain,
    gate_totals,
    conv_taps,
    attn_out_gain,
    conv_out_gain,
    attn_out_weight,
    conv_out_weight,
):
    return layer(
        tokens,
        mix_gain.reshape(1, -1),
        query_gain.reshape(1, -1),
        key_gain.reshape(1, -1),
        conv_taps,
        conv_out_gain.reshape(1, -1),
        gate_totals.T,
        attn_out_gain.reshape(1, -1),
        (
            query_weight,
            key_weight,
            value_weight,
            outer_gate_weight,
            inner_gate_weight,
            conv_input_weight,
            attn_out_weight,
            conv_out_weight,
        ),
        query_gain.shape[0],
    )


def solution(mesh):
    placed = (
        P("sp", "tp"),
        P(),
        P(None, "tp"),
        P(None, "tp"),
        P(None, "tp"),
        P(None, "tp"),
        P(None, "tp"),
        P(None, "tp"),
        P(),
        P(),
        P("sp", "tp"),
        P(None, "tp"),
        P("tp"),
        P("tp"),
        P("tp", None),
        P("tp", None),
    )
    return jax.shard_map(
        per_device, mesh=mesh, in_specs=placed, out_specs=P(("sp", "tp"), None), check_vma=False
    )
```

```python
import functools

import jax
import jax.numpy as jnp
from jax import lax
from jax.experimental import pallas as pl
from jax.experimental.pallas import tpu as pltpu
from jax.sharding import PartitionSpec as P

NORM_EPSILON = 1e-06
MESH = pl.DeviceIdType.MESH
CORES = 2
LANES = 128
VMEM = pltpu.VMEM


def greet(devices):
    barrier = pltpu.get_barrier_semaphore()
    for sp, tp in devices:
        pl.semaphore_signal(barrier, inc=1, device_id=(sp, tp), device_id_type=MESH)
    pl.semaphore_wait(barrier, len(devices))


def mesh_copy(src, dst, send, recv, device):
    return pltpu.make_async_remote_copy(
        src, dst, send, recv, device_id=device, device_id_type=MESH
    )


def layer_kernel(
    plan, tokens_ref, mix_ref, query_gain_ref, key_gain_ref, taps_ref, conv_gain_ref, gates_ref,
    attn_gain_ref, *refs
):
    sp_count, tp_count, head_count, head_dim, piece = plan
    weight_refs = refs[:8]
    out_ref = refs[8]
    (
        weights, out_weights, gathered, scaled, row_scales, kv_send, query_send,
        side_send, outer, padded, edge_send, edge_recv, kv_in, query_in, side_in, conv_mixed,
        conv_in, done, landed, rhs, gates, scores_a, scores_b, conv_rows,
        weight_sem, own_sem, cross_send, mate_send, tok_pass_send, tok_recv,
        kv_ssem, kv_rsem, query_ssem, query_rsem, side_ssem, side_rsem,
        kv_psem, kv_prsem, side_psem, side_prsem, local, edge_sem,
        send, recv, conv_ssem, conv_rsem, out_recv, out_cross, out_side, out_mate,
    ) = refs[9:]
    f32 = jnp.float32
    bf16 = jnp.bfloat16
    sp = lax.axis_index("sp")
    tp = lax.axis_index("tp")
    core = lax.rem(tp, CORES)
    mate = tp + 1 - 2 * core
    first = tp - core
    chips = tp_count // CORES
    targets = sp_count // CORES
    rows, features = tokens_ref.shape
    width = head_count * head_dim
    half = LANES
    chunk = 2 * half
    chunks = rows // chunk
    pieces = rows // piece
    share = pieces // CORES
    phases = min(2, piece // half)
    tile = piece // phases
    slabs = piece // half
    span = 256
    both_tiles = 2 * tile
    block_rows = rows // tp_count
    parts = 4
    part_rows = width // parts
    parity = lax.rem(sp, 2)
    beside = sp + 1 - 2 * parity
    order = [chunks - 1] + list(range(chunks - 1))
    home = sp // targets
    head_slot = (first + home) * head_count + lax.rem(sp, targets) // share
    owner = home == core
    place_here = lax.rem(sp, share) * CORES + core
    query_gain = jnp.concatenate([query_gain_ref[...]] * head_count, axis=1)
    key_gain = jnp.concatenate([key_gain_ref[...]] * head_count, axis=1)

    mine = pltpu.make_async_copy(tokens_ref, gathered.at[tp], own_sem)
    mine.start()
    loads = [
        pltpu.make_async_copy(
            ref,
            weights.at[index]
            if index < 6
            else out_weights.at[index - 6, pl.ds(pl.multiple_of(tp * width, width), width)],
            weight_sem.at[index],
        )
        for index, ref in enumerate(weight_refs)
    ]
    for index in (1, 2, 0, 3, 4, 5, 6, 7):
        loads[index].start()
    padded[0:8, :] = jnp.zeros((8, width), f32)
    for head in range(head_count):
        lines = [
            gates_ref[head : head + 1, row * LANES : (row + 1) * LANES]
            for row in range(rows // LANES)
        ]
        gain_line = attn_gain_ref[:, head * head_dim : (head + 1) * head_dim]
        gain_line = jnp.concatenate([gain_line, jnp.zeros((1, LANES - head_dim), f32)], axis=1)
        lines.append(jnp.broadcast_to(gain_line, (8, LANES)))
        side_send[head, :, :] = jnp.concatenate(lines, axis=0)
    greet(
        [
            (lax.rem(sp + step, sp_count), lax.rem(tp + other, tp_count))
            for step in range(sp_count)
            for other in range(tp_count)
            if step or other
        ]
    )

    def block(number):
        return pl.ds(number * chunk, chunk)

    def tokens_to(device, number, sem):
        return mesh_copy(
            gathered.at[tp, block(number)], gathered.at[tp, block(number)], sem,
            tok_recv.at[tp, number], device,
        )

    def to_mate_tokens(number):
        return tokens_to((sp, mate), number, mate_send.at[number])

    def across_tokens(step, number):
        return tokens_to(
            (sp, lax.rem(tp + CORES * step, tp_count)), number, cross_send.at[step - 1, number]
        )

    def token_pass(step, number):
        other = lax.rem(tp + CORES * step, tp_count)
        return mesh_copy(
            gathered.at[other, block(number)], gathered.at[other, block(number)],
            tok_pass_send.at[step - 1, number], tok_recv.at[other, number], (sp, mate),
        )

    def token_arrival(source, number):
        return mesh_copy(
            gathered.at[source, block(number)], gathered.at[source, block(number)],
            mate_send.at[number], tok_recv.at[source, number], (sp, mate),
        )

    mine.wait()
    for number in order:
        for step in range(1, chips):
            across_tokens(step, number).start()
        to_mate_tokens(number).start()

    def target_of(step):
        at = lax.rem(sp + 1 + step, targets)
        return at // share, core * targets + at

    def side_copy(step, head, target):
        return mesh_copy(
            side_send.at[head], side_in.at[sp], side_ssem.at[step], side_rsem.at[sp], (target, tp)
        )

    def kv_copy(step, number, head, target):
        return mesh_copy(
            kv_send.at[head, block(number)], kv_in.at[sp, block(number)],
            kv_ssem.at[step, number], kv_rsem.at[sp, number], (target, tp),
        )

    def kept(number, head):
        return pltpu.make_async_copy(
            kv_send.at[head, block(number)], kv_in.at[sp, block(number)], local.at[number]
        )

    def kept_side(head):
        return pltpu.make_async_copy(side_send.at[head], side_in.at[sp], local.at[chunks])

    def slab_copies(slab, starting):
        spot, inner = slab // slabs, slab % slabs
        place = jnp.where(lax.rem(sp, 2) == 0, spot, pieces - 1 - spot)
        part = pl.ds(slab * head_dim, head_dim)
        for step in range(head_count):
            head = lax.rem(sp + 1 + step, head_count)
            target = core * targets + head * share + place // CORES
            there = first + lax.rem(place, CORES)
            here = jnp.logical_and(target == sp, there == tp)

            if starting:

                @pl.when(here)
                def _():
                    pltpu.make_async_copy(
                        query_send.at[head, part], query_in.at[sp, inner],
                        query_rsem.at[sp, inner],
                    ).start()

            @pl.when(jnp.logical_not(here))
            def _():
                copy = mesh_copy(
                    query_send.at[head, part], query_in.at[sp, inner],
                    query_ssem.at[step, slab], query_rsem.at[sp, inner], (target, there),
                )
                if starting:
                    copy.start()
                else:
                    copy.wait_send()

    def query_arrival(source, inner):
        mesh_copy(
            query_send.at[0, pl.ds(0, head_dim)], query_in.at[source, inner],
            query_ssem.at[0, 0], query_rsem.at[source, inner], (sp, mate),
        ).wait_recv()

    for step in range(targets):
        head, target = target_of(step)

        @pl.when(target != sp)
        def _():
            side_copy(step, head, target).start()

        @pl.when(target == sp)
        def _():
            kept_side(head).start()

    ones_row = lax.broadcasted_iota(jnp.int32, (width, width), 0) // head_dim
    ones_column = lax.broadcasted_iota(jnp.int32, (width, width), 1) // head_dim
    spread_mean = jnp.where(ones_row == ones_column, 1.0 / head_dim, 0.0).astype(bf16)

    def normed(values, gain):
        squares = values * values
        high = squares.astype(bf16)
        low = (squares - high.astype(f32)).astype(bf16)
        mean = jnp.dot(high, spread_mean, preferred_element_type=f32)
        mean = mean + jnp.dot(low, spread_mean, preferred_element_type=f32)
        return values * lax.rsqrt(mean + NORM_EPSILON) * gain

    def project(number, index):
        product = jnp.dot(
            scaled[block(number), :], weights[index], preferred_element_type=f32
        )
        return product * row_scales[block(number), 0:1]

    def take_tokens(number):
        here = block(number)
        for step in range(1, chips):
            token_arrival(lax.rem(tp + CORES * step, tp_count), number).wait_recv()
            token_pass(step, number).start()
        token_arrival(mate, number).wait_recv()
        for step in range(1, chips):
            token_arrival(lax.rem(mate + CORES * step, tp_count), number).wait_recv()
        total = jnp.zeros((chunk, 1), f32)
        for source in range(tp_count):
            part = gathered[source, here, :].astype(f32)
            at = slice(source * features, (source + 1) * features)
            total = total + jnp.sum(part * part, axis=1, keepdims=True)
            scaled[here, at] = (part * mix_ref[:, at]).astype(bf16)
        row_scale = lax.rsqrt(total / (tp_count * features) + NORM_EPSILON)
        row_scales[here, :] = jnp.broadcast_to(row_scale, (chunk, LANES))

    def send_keys(number):
        keys = normed(project(number, 1), key_gain).astype(bf16)
        values = project(number, 2)
        for head in range(head_count):
            at = slice(head * head_dim, (head + 1) * head_dim)
            kv_send[head, pl.ds(number * chunk, half), :] = jnp.concatenate(
                [keys[:half, at], keys[half:, at]], axis=1
            )
        for side in range(2):
            rows_of = slice(side * half, (side + 1) * half)
            for lane in range(0, width, LANES):
                turned = values[rows_of, lane : lane + LANES].T.astype(bf16)
                for inner in range(LANES // head_dim):
                    kv_send[
                        lane // head_dim + inner,
                        pl.ds(number * chunk + half + side * head_dim, head_dim),
                        :,
                    ] = turned[inner * head_dim : (inner + 1) * head_dim]
        for step in range(targets):
            head, target = target_of(step)

            @pl.when(target != sp)
            def _():
                kv_copy(step, number, head, target).start()

            @pl.when(target == sp)
            def _():
                kept(number, head).start()

    def send_queries(number):
        queries = normed(project(number, 0), query_gain).astype(bf16)
        queries = queries.astype(f32) * head_dim ** (-0.5)
        for side in range(2):
            rows_of = slice(side * half, (side + 1) * half)
            for lane in range(0, width, LANES):
                turned = queries[rows_of, lane : lane + LANES].T.astype(bf16)
                for inner in range(LANES // head_dim):
                    query_send[
                        lane // head_dim + inner,
                        pl.ds(number * half + side * head_dim, head_dim),
                        :,
                    ] = turned[inner * head_dim : (inner + 1) * head_dim]
        slab_copies(2 * number, True)

    def part_of(kind, source, part):
        at = pl.multiple_of(source * width + part * part_rows, part_rows)
        return out_weights.at[kind, pl.ds(at, part_rows)]

    def weights_to(kind, source, part, sem, device):
        ref = part_of(kind, source, part)
        return mesh_copy(ref, ref, sem, out_recv.at[kind, source, part], device)

    def weights_across(step, part):
        return weights_to(
            parity, tp, part, out_cross.at[step - 1, part],
            (sp, lax.rem(tp + CORES * step, tp_count)),
        )

    def weights_last(step):
        return weights_to(
            1 - parity, tp, parts - 1, out_cross.at[step - 1, parts],
            (sp, lax.rem(tp + CORES * step, tp_count)),
        )

    def weights_beside(step, part):
        source = lax.rem(tp + CORES * step, tp_count)
        return weights_to(parity, source, part, out_side.at[step - 1, part], (beside, tp))

    def weights_mate(kind, source, part):
        return weights_to(kind, source, part, out_mate.at[kind, source, part], (sp, mate))

    def from_across(part):
        for step in range(1, chips):
            source = lax.rem(tp + CORES * step, tp_count)
            weights_mate(parity, source, part).wait_recv()
            if part < parts - 1:
                weights_beside(step, part).start()
            weights_mate(parity, source, part).start()

    def from_beside(part):
        for step in range(1, chips):
            source = lax.rem(tp + CORES * step, tp_count)
            weights_mate(1 - parity, source, part).wait_recv()
            weights_mate(1 - parity, source, part).start()

    def start_weights():
        loads[6].wait()
        loads[7].wait()
        for step in range(1, chips):
            for number in order:
                across_tokens(step, number).wait_send()
            for part in range(parts):
                weights_across(step, part).start()
            weights_last(step).start()

    sources = [lax.rem(sp + step, sp_count) for step in range(sp_count)]

    def kv_pass(source, number):
        return mesh_copy(
            kv_in.at[source, block(number)], kv_in.at[source, block(number)],
            kv_psem.at[source, number], kv_prsem.at[source, number], (sp, mate),
        )

    def side_pass(source):
        return mesh_copy(
            side_in.at[source], side_in.at[source], side_psem.at[source], side_prsem.at[source],
            (sp, mate),
        )

    def forward(number):
        @pl.when(owner)
        def _():
            for step, source in enumerate(sources):
                if step == 0:
                    kept(number, 0).wait()
                else:
                    mesh_copy(
                        kv_send.at[0, block(number)], kv_in.at[source, block(number)],
                        kv_ssem.at[0, number], kv_rsem.at[source, number], (sp, mate),
                    ).wait_recv()
                kv_pass(source, number).start()

    def pieces_of(values):
        high = values.astype(bf16).astype(f32)
        middle = (values - high).astype(bf16).astype(f32)
        low = (values - high - middle).astype(bf16).astype(f32)
        return high, middle, low

    def gate_columns(source, _):
        cuts = pieces_of(-side_in[source, : rows // LANES, :])
        for number in range(chunks):
            lines = [
                cut[2 * number + side : 2 * number + side + 1, :] for side in range(2) for cut in cuts
            ]
            lines.append(jnp.zeros((LANES - len(lines), LANES), f32))
            gates[source, number * half : (number + 1) * half, :] = (
                jnp.concatenate(lines, axis=0).T.astype(bf16)
            )
        return 0

    def conv_inputs(number):
        here = block(number)
        outer[here, :] = project(number, 3)
        gated = (project(number, 4) * project(number, 5)).astype(bf16)
        padded[pl.ds(8 + number * chunk, chunk), :] = gated.astype(f32)
        return gated

    edge = mesh_copy(
        edge_send, edge_recv, edge_sem.at[0], edge_sem.at[1], (lax.rem(sp + 1, sp_count), tp)
    )
    def take_sides():
        @pl.when(owner)
        def _():
            for step, source in enumerate(sources):
                if step == 0:
                    kept_side(0).wait()
                else:
                    mesh_copy(
                        side_send.at[0], side_in.at[source], side_ssem.at[0], side_rsem.at[source],
                        (sp, mate),
                    ).wait_recv()
                side_pass(source).start()

        @pl.when(jnp.logical_not(owner))
        def _():
            for source in sources:
                side_pass(source).wait_recv()

        lax.fori_loop(0, sp_count, gate_columns, 0)

    for index in (1, 2, 0, 3, 4, 5):
        loads[index].wait()
    for position, number in enumerate(order):
        take_tokens(number)
        send_keys(number)
        send_queries(number)
        if position == chunks - 1:
            for other in order:
                slab_copies(2 * other + 1, True)
            start_weights()
        gated = conv_inputs(number)
        if position == 0:
            edge_send[...] = gated[chunk - 16 :, :]

            @pl.when(sp < sp_count - 1)
            def _():
                edge.start()

            take_sides()
        if position > 1:
            forward(order[position - 2])
    gain_tile = jnp.broadcast_to(side_in[0, rows // LANES : rows // LANES + 1, :], (LANES, LANES))
    gain = gain_tile.T[:head_dim, 0:1]


    @pl.when(sp > 0)
    def _():
        edge.wait_recv()
        padded[0:8, :] = edge_recv[8:16, :].astype(f32)

    taps = taps_ref.shape[0]
    for number in range(chunks):
        convolved = jnp.zeros((chunk, width), f32)
        for tap in range(taps):
            at = pl.ds(8 - taps + 1 + tap + number * chunk, chunk)
            convolved = convolved + taps_ref[tap : tap + 1, :] * padded[at, :]
        conv_mixed[block(number), :] = normed(
            outer[block(number), :] * convolved, conv_gain_ref[...]
        ).astype(bf16)

    def conv_share(step):
        there = lax.rem(tp + step, tp_count)
        at = pl.ds(pl.multiple_of(there * block_rows, block_rows), block_rows)
        return mesh_copy(
            conv_mixed.at[at], conv_in.at[tp], conv_ssem.at[step - 1], conv_rsem.at[tp],
            (sp, there),
        )

    for step in range(1, tp_count):
        conv_share(step).start()
    own_rows = pl.ds(pl.multiple_of(tp * block_rows, block_rows), block_rows)
    conv_in[tp, :, :] = conv_mixed[own_rows, :]
    forward(order[-2])
    from_across(0)
    forward(order[-1])
    from_across(1)

    @pl.when(jnp.logical_not(owner))
    def _():
        for source in sources:
            for number in order:
                kv_pass(source, number).wait_recv()

    for kind in range(2):
        for part in range(parts):
            weights_mate(kind, tp, part).start()

    def place_of(phase, inner, spot):
        begin = (inner * phases + phase) * half
        return spot * (piece // block_rows) + begin // block_rows, begin % block_rows

    def away(phase, source, inner, spot):
        there, at = place_of(phase, inner, spot)
        return mesh_copy(
            done.at[phase, source, :, pl.ds(inner * half, half)],
            landed.at[head_slot, :, pl.ds(at, half)],
            send.at[phase, source, inner], recv.at[head_slot, at // half], (source, there),
        )

    def stays_here(phase, source, inner, spot):
        return jnp.logical_and(source == sp, place_of(phase, inner, spot)[0] == tp)

    even_spot, odd_spot = place_here, pieces - 1 - place_here

    def queries_of(phase, source):
        return jnp.concatenate(
            [query_in[source, slab, :, :] for slab in range(phase, slabs, phases)], axis=1
        )

    def set_queries(phase, even, odd):
        queries = jnp.concatenate([queries_of(phase, even), queries_of(phase, odd)], axis=1)
        empty = jnp.zeros_like(queries)
        row = lax.broadcasted_iota(jnp.int32, (LANES, both_tiles), 0)
        for side in range(2):
            ones = jnp.logical_and(row >= 3 * side, row < 3 * side + 3)
            stacked = [queries, empty] if side == 0 else [empty, queries]
            rhs[side, :, :] = jnp.concatenate(
                stacked + [jnp.where(ones, 1.0, 0.0).astype(bf16)], axis=0
            )

    def score(source, side, scores, top, limit):
        key_rows = jnp.concatenate(
            [kv_in[source, pl.ds(number * chunk, half), :] for number in range(rows // chunk)],
            axis=0,
        )
        lhs = jnp.concatenate([key_rows, gates[source, :, :]], axis=1)
        part = jnp.dot(lhs, rhs[side, :, :], preferred_element_type=f32)
        if limit is not None:
            row = lax.broadcasted_iota(jnp.int32, part.shape, 0)
            row = row // half * chunk + lax.rem(row, half) + side * half
            part = jnp.where(row <= limit, part, -jnp.inf)
        scores[side * (rows // 2) : (side + 1) * (rows // 2), :] = part
        return jnp.maximum(top, jnp.max(part.reshape(-1, 8, both_tiles), axis=0))

    def blend(source, scores, side, begin, top, total):
        start = side * (rows // 2) + begin * half
        weights = jnp.exp(scores[start : start + span, :] - top).astype(bf16)
        values = jnp.concatenate(
            [
                kv_in[source, pl.ds((begin + index) * chunk + half + side * head_dim, head_dim), :]
                for index in range(span // half)
            ],
            axis=1,
        )
        return total + jnp.dot(values, weights, preferred_element_type=f32)

    def start_top():
        return jnp.full((8, both_tiles), -jnp.inf, f32)

    def settle_top(top):
        return jnp.max(top, axis=0, keepdims=True)

    def advance(old, old_scores, old_top, state, new, new_scores, limit=None):
        top = jnp.maximum(state[0], old_top)
        total = state[1] * jnp.exp(state[0] - top)
        new_top = start_top()
        for side in range(2):
            if new is not None:
                new_top = score(new, side, new_scores, new_top, limit)
            for begin in range(0, rows // chunk, span // half):
                total = blend(old, old_scores, side, begin, top, total)
        return (top, total), settle_top(new_top)

    def finish(phase, source, attended, spot):
        scale = lax.rsqrt(jnp.mean(attended * attended, axis=0, keepdims=True) + NORM_EPSILON)
        done[phase, source, :, :] = (attended * scale * gain).astype(bf16)
        for inner in range(tile // half):
            stays = stays_here(phase, source, inner, spot)

            @pl.when(stays)
            def _():
                at = place_of(phase, inner, spot)[1]
                pltpu.make_async_copy(
                    done.at[phase, source, :, pl.ds(inner * half, half)],
                    landed.at[head_slot, :, pl.ds(at, half)],
                    recv.at[head_slot, at // half],
                ).start()

            @pl.when(jnp.logical_not(stays))
            def _():
                away(phase, source, inner, spot).start()

    def attend(phase):
        for source in range(sp_count):
            for inner in range(phase, slabs, phases):
                query_arrival(source, inner)
        column = lax.broadcasted_iota(jnp.int32, (1, both_tiles), 1)
        inside = lax.rem(column, tile)
        inside = (inside // half * phases + phase) * half + lax.rem(inside, half)
        in_even = column < tile
        even_limit = jnp.where(in_even, inside + even_spot * piece, rows)
        odd_limit = jnp.where(in_even, -1, inside + odd_spot * piece)
        empty = (
            jnp.full((1, both_tiles), -1e30, f32), jnp.zeros((head_dim, both_tiles), f32)
        )

        pairs = sp_count // 2

        def pair_at(index):
            return index + (index == pairs - 2) * 1 - (index == pairs - 1) * 1

        def pair_of_sources(index, carried):
            state, top, last = carried
            pair = pair_at(index)
            before = 2 * pair_at(index - 1)
            even, odd = 2 * pair, 2 * pair + 1
            set_queries(phase, even, odd)
            state, top = advance(last, scores_b, top, state, even, scores_a, even_limit)

            @pl.when(index > 0)
            def _():
                finish(phase, before, state[1][:, :tile], even_spot)
                finish(phase, before + 1, state[1][:, tile:], odd_spot)

            state, top = advance(even, scores_a, top, empty, odd, scores_b, odd_limit)

            def two_sources(step, carried):
                state, top, last = carried
                state, top = advance(last, scores_b, top, state, 2 * step, scores_a)
                state, top = advance(2 * step, scores_a, top, state, 2 * step + 1, scores_b)
                return state, top, 2 * step + 1

            return lax.fori_loop(0, pair, two_sources, (state, top, odd))

        if phase == 0:
            scores_b[...] = jnp.zeros_like(scores_b)
        carried = (empty, jnp.zeros((1, both_tiles), f32), 0)
        carried = lax.fori_loop(0, pairs - 1, pair_of_sources, carried)
        hook(phase)
        state, top, last = lax.fori_loop(pairs - 1, pairs, pair_of_sources, carried)
        state, _ = advance(last, scores_b, top, state, None, None)
        finish(phase, sp_count - 4, state[1][:, :tile], even_spot)
        finish(phase, sp_count - 3, state[1][:, tile:], odd_spot)

    def hook(phase):
        if phase == 0:
            from_across(2)
            from_across(3)
        if phase == phases - 1:
            for part in range(parts):
                from_beside(part)

    for phase in range(phases):
        attend(phase)
    for step in range(1, tp_count):
        source = lax.rem(tp + step, tp_count)
        mesh_copy(
            conv_mixed.at[pl.ds(0, block_rows)], conv_in.at[source], conv_ssem.at[0],
            conv_rsem.at[source], (sp, mate),
        ).wait_recv()
    for step in range(chips):
        source = lax.rem(mate + CORES * step, tp_count)
        for kind in range(2):
            for part in range(parts):
                weights_mate(kind, source, part).wait_recv()
    out_span = 512
    out_features = out_ref.shape[1]
    conv_rows_in = jnp.concatenate([conv_in[source, :, :] for source in range(tp_count)], axis=1)
    for begin in range(0, out_features, out_span):
        at = slice(begin, begin + out_span)
        conv_rows[:, at] = jnp.dot(
            conv_rows_in, out_weights[1, :, at], preferred_element_type=f32
        )
    for phase in range(phases):
        for index in range(phase, block_rows // half, phases):
            for source in range(tp_count * head_count):
                mesh_copy(
                    done.at[0, 0, :, pl.ds(0, half)],
                    landed.at[source, :, pl.ds(index * half, half)],
                    send.at[0, 0, 0], recv.at[source, index], (sp, mate),
                ).wait_recv()
            here = slice(index * half, (index + 1) * half)
            mixed = landed[:, :, here].reshape(tp_count * width, half)
            mixed = mixed.astype(f32).T.astype(bf16)
            for begin in range(0, out_features, out_span):
                at = slice(begin, begin + out_span)
                out_ref[here, at] = (
                    conv_rows[here, at]
                    + jnp.dot(mixed, out_weights[0, :, at], preferred_element_type=f32)
                ).astype(bf16)
    for phase in range(phases):
        for source in range(sp_count):
            for inner in range(tile // half):
                spot = odd_spot if source % 2 else even_spot

                @pl.when(jnp.logical_not(stays_here(phase, source, inner, spot)))
                def _():
                    away(phase, source, inner, spot).wait_send()

    for step in range(1, tp_count):
        conv_share(step).wait_send()
    for part in range(parts):
        for kind in range(2):
            for step in range(chips):
                weights_mate(kind, lax.rem(tp + CORES * step, tp_count), part).wait_send()
        for step in range(1, chips):
            weights_across(step, part).wait_send()
            if part < parts - 1:
                weights_beside(step, part).wait_send()
            else:
                weights_last(step).wait_send()

    @pl.when(owner)
    def _():
        for source in sources:
            side_pass(source).wait_send()
            for number in order:
                kv_pass(source, number).wait_send()

    for step in range(targets):
        head, target = target_of(step)

        @pl.when(target != sp)
        def _():
            side_copy(step, head, target).wait_send()
            for number in order:
                kv_copy(step, number, head, target).wait_send()

    for slab in range(2 * chunks):
        slab_copies(slab, False)
    for number in order:
        to_mate_tokens(number).wait_send()
        for step in range(1, chips):
            token_pass(step, number).wait_send()

    @pl.when(sp < sp_count - 1)
    def _():
        edge.wait_send()


def layer(
    tokens, mix_gain, query_gain, key_gain, taps, conv_gain, gate_rows, attn_gain, weights, head_dim
):
    sp_count = lax.axis_size("sp")
    tp_count = lax.axis_size("tp")
    rows, features = tokens.shape
    width = weights[0].shape[1]
    out_features = weights[6].shape[1]
    heads = width // head_dim
    pieces = sp_count // heads
    piece = rows // pieces
    phases = min(2, piece // LANES)
    tile = piece // phases
    slabs = piece // LANES
    chunks = rows // LANES // 2
    chips = tp_count // CORES
    targets = sp_count // CORES
    block_rows = rows // tp_count
    parts = 4
    links = max(chips - 1, 1)
    bf16 = jnp.bfloat16
    f32 = jnp.float32
    dma = pltpu.SemaphoreType.DMA
    vmem = pl.BlockSpec(memory_space=VMEM)
    hbm = pl.BlockSpec(memory_space=pl.ANY)
    return pl.pallas_call(
        functools.partial(layer_kernel, (sp_count, tp_count, heads, head_dim, piece)),
        out_shape=jax.ShapeDtypeStruct((block_rows, out_features), bf16),
        in_specs=[hbm] + [vmem] * 7 + [hbm] * 8,
        out_specs=vmem,
        scratch_shapes=[
            VMEM((6,) + weights[0].shape, bf16),
            VMEM((2, tp_count * width, out_features), bf16),
            VMEM((tp_count, rows, features), bf16),
            VMEM((rows, tp_count * features), bf16),
            VMEM((rows, LANES), f32),
            VMEM((heads, rows, LANES), bf16),
            VMEM((heads, rows // 2, LANES), bf16),
            VMEM((heads, rows // LANES + 8, LANES), f32),
            VMEM((rows, width), f32),
            VMEM((rows + 8, width), f32),
            VMEM((16, width), bf16),
            VMEM((16, width), bf16),
            VMEM((sp_count, rows, LANES), bf16),
            VMEM((sp_count, slabs, head_dim, LANES), bf16),
            VMEM((sp_count, rows // LANES + 8, LANES), f32),
            VMEM((rows, width), bf16),
            VMEM((tp_count, block_rows, width), bf16),
            VMEM((phases, sp_count, head_dim, tile), bf16),
            VMEM((tp_count * heads, head_dim, block_rows), bf16),
            VMEM((2, 2 * LANES, 2 * tile), bf16),
            VMEM((sp_count, rows // 2, LANES), bf16),
            VMEM((rows, 2 * tile), f32),
            VMEM((rows, 2 * tile), f32),
            VMEM((block_rows, out_features), f32),
            dma((8,)), dma, dma((links, chunks)), dma((chunks,)), dma((links, chunks)),
            dma((tp_count, chunks)),
            dma((targets, chunks)), dma((sp_count, chunks)),
            dma((heads, 2 * chunks)), dma((sp_count, slabs)),
            dma((targets,)), dma((sp_count,)),
            dma((sp_count, chunks)), dma((sp_count, chunks)),
            dma((sp_count,)), dma((sp_count,)),
            dma((chunks + 1,)), dma((2,)),
            dma((phases, sp_count, tile // LANES)), dma((tp_count * heads, block_rows // LANES)),
            dma((tp_count - 1,)), dma((tp_count,)),
            dma((2, tp_count, parts)), dma((links, parts + 1)), dma((links, parts)),
            dma((2, tp_count, parts)),
        ],
        compiler_params=pltpu.CompilerParams(
            collective_id=0, has_side_effects=True, vmem_limit_bytes=63 * 1024 * 1024
        ),
    )(tokens, mix_gain, query_gain, key_gain, taps, conv_gain, gate_rows, attn_gain, *weights)


def per_device(
    tokens,
    mix_gain,
    query_weight,
    key_weight,
    value_weight,
    outer_gate_weight,
    inner_gate_weight,
    conv_input_weight,
    query_gain,
    key_gain,
    gate_totals,
    conv_taps,
    attn_out_gain,
    conv_out_gain,
    attn_out_weight,
    conv_out_weight,
):
    return layer(
        tokens,
        mix_gain.reshape(1, -1),
        query_gain.reshape(1, -1),
        key_gain.reshape(1, -1),
        conv_taps,
        conv_out_gain.reshape(1, -1),
        gate_totals.T,
        attn_out_gain.reshape(1, -1),
        (
            query_weight,
            key_weight,
            value_weight,
            outer_gate_weight,
            inner_gate_weight,
            conv_input_weight,
            attn_out_weight,
            conv_out_weight,
        ),
        query_gain.shape[0],
    )


def solution(mesh):
    placed = (
        P("sp", "tp"),
        P(),
        P(None, "tp"),
        P(None, "tp"),
        P(None, "tp"),
        P(None, "tp"),
        P(None, "tp"),
        P(None, "tp"),
        P(),
        P(),
        P("sp", "tp"),
        P(None, "tp"),
        P("tp"),
        P("tp"),
        P("tp", None),
        P("tp", None),
    )
    return jax.shard_map(
        per_device, mesh=mesh, in_specs=placed, out_specs=P(("sp", "tp"), None), check_vma=False
    )
```
